32 devices in a mesh: sp: 8 (over z, y), tp: 4 (over x, core).
Axes of the slice: x: 2, y: 2, z: 4, core: 2. Of those that a mesh axis runs over, the one named last changes fastest.
Arguments:
- tokens: bfloat16 [2048, 4096], P(('sp', 'tp')), may hold values from -6 to 6
- norm_gain: float32 [4096], replicated, may hold values from 0.1 to 1.9
- w_query: bfloat16 [4096, 1024], P(None, 'tp'), may hold values from -0.25 to 0.25
- w_key: bfloat16 [4096, 512], P(None, 'tp'), may hold values from -0.09375 to 0.09375
- w_value: bfloat16 [4096, 512], P(None, 'tp'), may hold values from -0.09375 to 0.09375
- score_shift: float32 [8], P('tp'), may hold values from -15 to -8
- w_conv_b: bfloat16 [4096, 1024], P(None, 'tp'), may hold values from -0.09375 to 0.09375
- w_conv_c: bfloat16 [4096, 1024], P(None, 'tp'), may hold values from -0.09375 to 0.09375
- w_conv_u: bfloat16 [4096, 1024], P(None, 'tp'), may hold values from -0.09375 to 0.09375
- conv_kernel: float32 [3, 1024], P(None, 'tp'), may hold values from -3.5 to 3.5
- w_out_att: bfloat16 [4096, 1024], P('sp', 'tp'), may hold values from -0.75 to 0.75
- w_out_conv: bfloat16 [4096, 1024], P('sp', 'tp'), may hold values from -0.1875 to 0.1875
Outputs:
- mixed: bfloat16 [2048, 4096], P(('sp', 'tp'))
- log_weight: float32 [2048, 8], P('sp', 'tp')
The draws below stay inside these ranges and needn't reach their ends.
All inputs are finite; a program needn't handle non-finite values.
Results may differ from the reference program's by a relative error of at most 0.017.
Values may be sent and summed in bfloat16 or wider, within the bound.
A program may use at most 128 MiB of HBM per device.

```python
import jax
import jax.numpy as jnp
from jax import lax

D = 4096
ATT_HEADS = 8
KV_HEADS = 4
HEAD_DIM = 128
CONV_W = 1024
CONV_K = 3
KEY_BLOCK = 1024
TOK_DEV = 256
ATT_W = 1024
TOKENS = 2048
N_TP = 4


def draw_score_shift(key, part):
    return jax.random.uniform(key, (ATT_HEADS,), jnp.float32, -13.0, -8.0)


def levels(rng, extent, shards, low, high):
    factor_of, own = 1.0, jax.random.fold_in(rng, 6)
    for position, blocks in shards:
        heights = jnp.exp(jax.random.uniform(jax.random.fold_in(own, position), (blocks,), jnp.float32, low / len(shards), high / len(shards)))
        factor_of = factor_of * jnp.repeat(heights, extent[position] // blocks).reshape([-1 if axis == position else 1 for axis in range(len(extent))])
    return factor_of


def bell_draw(key, extent, spread, most, split=(), kind=jnp.bfloat16):
    gain = levels(key, extent, split, -0.22, 0.18) if split else 1.0
    entries = jax.random.normal(key, extent, jnp.float32) * spread * gain
    return jnp.minimum(jnp.maximum(entries, -most), most).astype(kind)


def setup_inputs(seed: int = 0) -> dict:
    splits = jax.random.split(jax.random.key(seed), 13)
    tokens = bell_draw(splits[0], (TOKENS, D), 1.0, 6.0, ((0, 32),))
    norm_gain = jnp.clip(1.0 + 0.18 * jax.random.normal(splits[1], (D,), jnp.float32), 0.1, 1.9)
    w_query = bell_draw(splits[2], (D, ATT_W), (D // 9) ** -0.5, 0.25, ((1, 4),))
    w_key = bell_draw(splits[3], (D, KV_HEADS * HEAD_DIM), D ** -0.5, 0.09375, ((1, 4),))
    w_value = bell_draw(splits[4], (D, KV_HEADS * HEAD_DIM), D ** -0.5, 0.09375, ((1, 4),))
    score_shift = draw_score_shift(jax.random.fold_in(splits[12], 71), 0)
    w_conv_b = bell_draw(splits[6], (D, CONV_W), D ** -0.5, 0.09375, ((1, 4),))
    w_conv_c = bell_draw(splits[7], (D, CONV_W), D ** -0.5, 0.09375, ((1, 4),))
    w_conv_u = bell_draw(splits[8], (D, CONV_W), D ** -0.5, 0.09375, ((1, 4),))
    conv_kernel = bell_draw(splits[9], (CONV_K, CONV_W), CONV_K ** -0.5, 3.5, ((1, 4),), jnp.float32)
    w_out_att = bell_draw(splits[10], (D, ATT_W), (ATT_W // 16) ** -0.5, 0.75, ((0, 8), (1, 4)))
    w_out_conv = bell_draw(splits[11], (D, CONV_W), CONV_W ** -0.5, 0.1875, ((0, 8), (1, 4)))
    return {"tokens": tokens, "norm_gain": norm_gain, "w_query": w_query, "w_key": w_key, "w_value": w_value, "score_shift": score_shift, "w_conv_b": w_conv_b, "w_conv_c": w_conv_c, "w_conv_u": w_conv_u, "conv_kernel": conv_kernel, "w_out_att": w_out_att, "w_out_conv": w_out_conv}


def normalize(tokens, norm_gain):
    widened = tokens.astype(jnp.float32)
    inverse = lax.rsqrt(lax.optimization_barrier(jnp.mean(widened * widened, axis=-1, keepdims=True)) + 1e-06)
    return (widened * inverse * norm_gain).astype(jnp.bfloat16)

def block_terms(grouped_q, key_block, value_block, shifts, query_pos, key_first):
    scores = jnp.einsum('qhgd,khd->qhgk', grouped_q.astype(jnp.float32), key_block.astype(jnp.float32))
    scores = scores * HEAD_DIM ** (-0.5) + shifts[None, :, :, None]
    key_pos = key_first + jnp.arange(KEY_BLOCK, dtype=jnp.int32)
    causal = key_pos[None, None, None, :] < query_pos[:, None, None, None]
    soft = jnp.where(causal, jax.nn.softplus(scores), 0.0)
    after_sum = lax.cumsum(soft, axis=3, reverse=True) - soft
    relative = jnp.where(causal, jnp.exp(jax.nn.log_sigmoid(scores) - after_sum), 0.0).astype(jnp.bfloat16)
    partial_value = jnp.einsum('qhgk,khd->qhgd', relative.astype(jnp.float32), value_block.astype(jnp.float32))
    return (partial_value, lax.optimization_barrier(jnp.sum(soft, axis=3)))

def reference(tokens, norm_gain, w_query, w_key, w_value, score_shift, w_conv_b, w_conv_c, w_conv_u, conv_kernel, w_out_att, w_out_conv):
    normed = normalize(tokens, norm_gain)

    def project(weight):
        return jnp.dot(normed, weight, preferred_element_type=jnp.float32).astype(jnp.bfloat16)
    queries = project(w_query)
    keys = project(w_key)
    values = project(w_value)
    gate_b = project(w_conv_b)
    gate_c = project(w_conv_c)
    inputs_u = project(w_conv_u)
    grouping = ATT_HEADS // KV_HEADS
    shifts = score_shift.reshape(KV_HEADS, grouping)
    key_blocks = keys.reshape(TOKENS // KEY_BLOCK, KEY_BLOCK, KV_HEADS, HEAD_DIM)
    value_blocks = values.reshape(TOKENS // KEY_BLOCK, KEY_BLOCK, KV_HEADS, HEAD_DIM)
    key_firsts = jnp.arange(TOKENS // KEY_BLOCK, dtype=jnp.int32) * KEY_BLOCK
    query_blocks = queries.reshape(TOKENS // TOK_DEV, TOK_DEV, KV_HEADS, grouping, HEAD_DIM)
    query_firsts = jnp.arange(TOKENS // TOK_DEV, dtype=jnp.int32) * TOK_DEV

    def per_query(inputs):
        grouped_q, query_first = inputs
        query_pos = query_first + jnp.arange(TOK_DEV, dtype=jnp.int32)

        def per_key(key_inputs):
            key_block, value_block, key_first = key_inputs
            return block_terms(grouped_q, key_block, value_block, shifts, query_pos, key_first)
        partials, totals = lax.map(per_key, (key_blocks, value_blocks, key_firsts))
        later_sum = lax.cumsum(totals, axis=0, reverse=True) - totals
        attended = lax.optimization_barrier(jnp.sum(jnp.exp(-later_sum)[..., None] * partials, axis=0))
        sums_all = lax.optimization_barrier(jnp.sum(totals, axis=0))
        return (attended.reshape(TOK_DEV, ATT_W), sums_all.reshape(TOK_DEV, ATT_HEADS))
    attended, sums_all = lax.map(per_query, (query_blocks, query_firsts))
    attended = attended.reshape(TOKENS, ATT_W).astype(jnp.bfloat16)
    log_weight = jnp.log(jnp.maximum(-jnp.expm1(-sums_all.reshape(TOKENS, ATT_HEADS)), 0.05))
    products = (gate_c.astype(jnp.float32) * inputs_u.astype(jnp.float32)).astype(jnp.bfloat16)
    padded = jnp.concatenate([jnp.zeros((CONV_K - 1, CONV_W), jnp.bfloat16), products], axis=0)
    summed = jnp.zeros((TOKENS, CONV_W), jnp.float32)
    for tap in range(CONV_K):
        summed = summed + conv_kernel[tap][None, :] * padded[tap:tap + TOKENS].astype(jnp.float32)
    convolved = (gate_b.astype(jnp.float32) * summed).astype(jnp.bfloat16)
    att_cols = ATT_W // N_TP
    conv_cols = CONV_W // N_TP
    contract = (((1,), (1,)), ((), ()))
    mixed_sum = jnp.zeros((TOKENS, D), jnp.float32)
    for shard_no in range(N_TP):
        att_part = attended[:, shard_no * att_cols:(shard_no + 1) * att_cols]
        att_rows = w_out_att[:, shard_no * att_cols:(shard_no + 1) * att_cols]
        conv_part = convolved[:, shard_no * conv_cols:(shard_no + 1) * conv_cols]
        conv_rows = w_out_conv[:, shard_no * conv_cols:(shard_no + 1) * conv_cols]
        share = lax.dot_general(att_part, att_rows, contract, preferred_element_type=jnp.float32)
        share = share + lax.dot_general(conv_part, conv_rows, contract, preferred_element_type=jnp.float32)
        mixed_sum = mixed_sum + share.astype(jnp.bfloat16).astype(jnp.float32)
    return (mixed_sum.astype(jnp.bfloat16), log_weight)
```

```python
import functools

import jax
import jax.numpy as jnp
from jax import lax
from jax.experimental import pallas as pl
from jax.experimental.pallas import tpu as pltpu
from jax.sharding import PartitionSpec as P

HEAD_DIM = 128
CONV_K = 3
HALO = 16
F32 = jnp.float32
BF16 = jnp.bfloat16
MESH = pl.DeviceIdType.MESH
NT = (((1,), (1,)), ((), ()))
W_OWN = [(5, 1, 6, 7, 7, 3, 6, 2), (5, 5, 4, 7, 3, 3, 6, 6), (5, 5, 7, 7, 7, 5, 6, 6), (5, 5, 7, 6, 3, 7, 6, 6)]
W_EVENTS = [[],
 [],
 [(73, 1, 1, 68, 386, 193, 260, 324), (132, 192, 195, 129, -1, 258, 458, 386), (-1, -1, 256, 326, -1, 454, -1, -1)],
 [],
 [],
 [(81, 9, 8, 73, 394, 205, 268, 332),
  (148, 204, 200, 139, 338, 458, -1, 394),
  (89, 212, 270, 334, -1, -1, -1, -1),
  (156, -1, 278, 350, -1, -1, -1, -1)],
 [(192, 17, 208, 144, 402, 272, 466, 340),
  (200, 216, 286, 258, 149, 466, 276, -1),
  (-1, 24, 16, 80, 344, -1, 474, -1),
  (-1, -1, 219, -1, -1, -1, -1, -1)],
 [],
 [(208, 324, 384, 152, 410, 209, -1, 402), (268, -1, -1, 452, 157, 474, -1, -1), (-1, -1, -1, -1, 449, -1, -1, -1)],
 [(-1, 128, 28, 88, -1, -1, 284, 348), (-1, -1, 67, -1, -1, -1, -1, -1)],
 [(-1, -1, -1, -1, -1, -1, 322, -1)],
 [(276, 140, 392, 264, 456, 145, -1, 410), (-1, -1, -1, 460, 4, 133, -1, -1), (-1, -1, -1, -1, 200, 386, -1, -1)],
 [(-1, 144, 72, 0, -1, -1, 144, 192), (-1, -1, 320, -1, -1, -1, 330, -1)],
 [(-1, 332, 338, 272, 466, 76, -1, 256), (-1, -1, -1, 464, -1, 394, -1, -1)],
 [(-1, -1, -1, -1, 193, -1, -1, -1)],
 [(-1, -1, -1, 9, -1, -1, -1, 204)],
 [(-1, -1, -1, -1, 129, 141, -1, 266)],
 [(-1, -1, -1, -1, -1, 152, -1, -1)],
 [],
 [],
 [(320, -1, 81, -1, -1, -1, 156, -1), (-1, -1, 328, -1, -1, -1, 336, -1)],
 [(280, -1, -1, 282, -1, -1, -1, -1), (136, -1, -1, 472, -1, -1, -1, -1)],
 [(216, 152, -1, -1, 474, 402, 448, -1)],
 [(328, -1, 400, 17, 72, 0, 344, 212),
  (64, -1, -1, -1, 320, 408, -1, 144),
  (-1, -1, -1, -1, 136, -1, -1, 272),
  (-1, -1, -1, -1, 221, -1, -1, 128),
  (-1, -1, -1, -1, -1, -1, -1, 282)],
 [(344, 348, 89, -1, 328, 264, 192, 140),
  (340, 260, 344, -1, -1, 12, 200, 152),
  (-1, 264, -1, -1, -1, 216, 128, -1),
  (-1, 272, -1, -1, -1, -1, 210, -1),
  (-1, 280, -1, -1, -1, -1, 220, -1)],
 [(256, 337, -1, 384, 68, 20, 136, 216),
  (-1, -1, -1, 25, 84, 64, -1, -1),
  (-1, -1, -1, 392, 8, 28, -1, -1),
  (-1, -1, -1, -1, 92, -1, -1, -1)],
 [(-1, -1, 412, 400, 16, 280, -1, -1), (-1, -1, -1, 408, 208, -1, -1, -1)],
 [(-1, -1, 448, 336, 24, 80, -1, -1),
  (-1, -1, 464, -1, -1, 88, -1, -1),
  (-1, -1, 456, -1, -1, -1, -1, -1),
  (-1, -1, 472, -1, -1, -1, -1, -1)],
 [],
 []]
CELLS = [(0, 1, 2, 3, 4, 5, 6, 7),
 (2, 3, 4, 2, 6, 7, 4, 5),
 (3, 0, 3, 1, 7, 2, 7, 6),
 (1, 2, 0, 4, 2, 6, 5, 4),
 (5, 4, 1, 7, 5, 3, 3, 2),
 (4, 5, 5, 0, 1, 0, 2, 3),
 (-1, -1, 6, 6, 3, 4, -1, -1),
 (-1, -1, 7, 5, 0, 1, -1, -1),
 (-1, -1, 6, 6, 0, 0, -1, -1),
 (-1, -1, 7, 7, 1, 1, -1, -1)]
CELL_BACK = [(6, 6, -1, -1, -1, -1, 0, 0), (7, 7, -1, -1, -1, -1, 1, 1)]
CELL_ORDER = (0, 1, 2, 3, 4, 5, 6, 7, 8, 9)


def softplus(z):
    u = jnp.exp(-jnp.abs(z))
    small = u * (1.0 - u * (0.5 - u * (1.0 / 3.0 - u * 0.25)))
    return jnp.maximum(z, 0.0) + jnp.where(u < 0.01, small, jnp.log(1.0 + u))


def kernel(
    n,
    tok_ref, gain_ref, wq_hbm, wk_hbm, wv_hbm, shift_ref, wb_hbm, wc_hbm, wu_hbm, taps_ref, woa_ref, woc_ref,
    out_ref, logw_ref,
    wq, wk, wv, wb, wc, wu, xall, normed, q_sc, kv, wo, gate_sc, prod_sc, prev, ext, attn, conv, partial, totals,
    snd, keep, d2d, xsnd, xrcv,
    load_sem, tok_ssem, tok_rsem, kv_sem, w_sem, halo_sem, d2d_sem, x_sem,
):
    sp = lax.axis_index("sp")
    t = lax.axis_index("tp")
    near = t + 1 - 2 * (t % 2)
    far = t + 2 - 4 * ((t // 2) % 2)
    diag = near + 2 - 4 * ((near // 2) % 2)
    pos = jnp.where(sp % 2 == 0, sp // 2, n - 1 - sp // 2)

    def ring(place):
        place = (place + 2 * n) % n
        return jnp.where(place < n // 2, 2 * place, 2 * (n - 1 - place) + 1)

    right, left = ring(pos + 1), ring(pos - 1)
    following, leading = (sp + 1) % n, (sp + n - 1) % n
    rows = tok_ref.shape[0]
    toks = 4 * rows
    half = rows // 2
    fpart = wo.shape[2] // 2
    heads = q_sc.shape[1] // HEAD_DIM
    kv_cols = kv.shape[4]
    grouping = heads // (kv_cols // HEAD_DIM)

    loads = [
        pltpu.make_async_copy(src, dst, load_sem.at[i])
        for i, (src, dst) in enumerate(
            ((wk_hbm, wk), (wv_hbm, wv), (wq_hbm, wq), (wc_hbm, wc), (wu_hbm, wu), (wb_hbm, wb))
        )
    ]
    own_loads = [
        pltpu.make_async_copy(src, wo.at[sp, i], load_sem.at[6 + i]) for i, src in enumerate((woa_ref, woc_ref))
    ]
    barrier = pltpu.get_barrier_semaphore()
    for place in (right, left, following, leading):
        pl.semaphore_signal(barrier, inc=1, device_id={"sp": place}, device_id_type=MESH)
    for place in (near, far):
        pl.semaphore_signal(barrier, inc=1, device_id={"tp": place}, device_id_type=MESH)
    for load in (*own_loads, *loads):
        load.start()
    pl.semaphore_wait(barrier, 6)

    def push(src, dst, ssem, rsem, who):
        return pltpu.make_async_remote_copy(
            src_ref=src, dst_ref=dst, send_sem=ssem, recv_sem=rsem, device_id=who, device_id_type=MESH
        )

    to_far = [
        push(tok_ref.at[pl.ds(c * half, half)], xall.at[t, pl.ds(c * half, half)], tok_ssem.at[c], tok_rsem.at[c], {"tp": far})
        for c in range(2)
    ]
    to_near = push(tok_ref, xall.at[t], tok_ssem.at[2], tok_rsem.at[2], {"tp": near})
    relay = [
        push(xall.at[far, pl.ds(c * half, half)], xall.at[far, pl.ds(c * half, half)], tok_ssem.at[3 + c], tok_rsem.at[3 + c], {"tp": near})
        for c in range(2)
    ]
    for copy in to_far:
        copy.start()
    to_near.start()

    last = n // 2

    def hop(part, sem, way, step, chunk):
        block = ring(pos - (step - 1)) if way == 0 else ring(pos + (step - 1))
        view = part(block, chunk, step)
        return push(
            view[0], view[1], sem.at[0, way, step - 1, chunk], sem.at[1, way, step - 1, chunk],
            {"sp": right if way == 0 else left},
        )

    def ways(step, chunk, chunks):
        if isinstance(step, int) and step == last:
            return (0,) if chunk < chunks // 2 else (1,)
        return (0, 1)

    early = t // 2

    def kv_part(block, chunk, step):
        view = kv.at[block, early + chunk * (1 - 2 * early)]
        return view, view

    def w_part(block, chunk, step):
        view = wo.at[block, chunk // 2, pl.ds(pl.multiple_of((chunk % 2) * fpart, fpart), fpart)]
        return view, view

    rings = {"kv": (kv_part, kv_sem, 2), "w": (w_part, w_sem, 4)}

    def emit(name, step, chunk):
        part, sem, chunks = rings[name]
        for way in ways(step, chunk, chunks):
            hop(part, sem, way, step, chunk).start()

    def take(name, step, chunk, onward=None):
        part, sem, chunks = rings[name]
        for way in ways(step, chunk, chunks):
            hop(part, sem, way, step, chunk).wait_recv()
        if onward or (onward is None and step < last):
            emit(name, step + 1, chunk)

    for load in own_loads:
        load.wait()
    for chunk in (0, 1):
        emit("w", 1, chunk)

    def dot(w):
        return jnp.dot(normed[...], w[...], preferred_element_type=F32).astype(BF16)

    def project_kv(groups, pair):
        for i, g in enumerate(groups):
            x = (tok_ref[...] if g is None else xall[g]).astype(F32)
            inverse = lax.rsqrt(jnp.mean(x * x, axis=-1, keepdims=True) + 1e-06)
            at = rows * (t % 2 if i == 0 else 1 - t % 2)
            normed[pl.ds(pl.multiple_of(at, rows), rows)] = (x * inverse * gain_ref[...]).astype(BF16)
        kv[sp, pair, 0] = dot(wk)
        kv[sp, pair, 1] = dot(wv)

    def project_rest(pair):
        at = pl.ds(pl.multiple_of(pair * 2 * rows, 2 * rows), 2 * rows)
        prod_sc[at] = (dot(wc).astype(F32) * dot(wu).astype(F32)).astype(BF16)
        q_sc[at] = dot(wq)
        gate_sc[at] = dot(wb)

    to_near.wait_recv()
    for load in loads[:2]:
        load.wait()
    project_kv((None, near), early)
    emit("kv", 1, 0)
    for chunk in (2, 3):
        emit("w", 1, chunk)
    for load in loads[2:]:
        load.wait()
    project_rest(early)
    to_far[0].wait_recv()
    relay[0].start()
    take("kv", 1, 0)
    take("w", 1, 0)
    to_far[1].wait_recv()
    relay[1].start()
    for c in range(2):
        relay[c].wait_recv()
    project_kv((far, diag), 1 - early)
    emit("kv", 1, 1)
    take("w", 1, 1)
    take("w", 1, 2)
    project_rest(1 - early)
    halo = push(prod_sc.at[pl.ds(toks - HALO, HALO)], prev, halo_sem.at[0], halo_sem.at[1], {"sp": following})
    halo.start()

    key_i = lax.broadcasted_iota(jnp.int32, (toks, toks), 0)
    key_j = lax.broadcasted_iota(jnp.int32, (toks, toks), 1)
    later = (key_i > key_j).astype(F32).astype(BF16)
    lane = lax.broadcasted_iota(jnp.int32, (toks, totals.shape[2]), 1)
    scale = HEAD_DIM ** (-0.5)
    order = (t, far, near, diag)

    def visit(slot, masked):
        for h in range(heads):
            cols = pl.ds(h * HEAD_DIM, HEAD_DIM)
            kv_at = pl.ds((h // grouping) * HEAD_DIM, HEAD_DIM)
            keys = kv[slot, :, 0, :, kv_at].reshape(toks, HEAD_DIM)
            vals = kv[slot, :, 1, :, kv_at].reshape(toks, HEAD_DIM)
            z = lax.dot_general(q_sc[:, cols], keys, NT, preferred_element_type=F32) * scale + shift_ref[0, h]
            soft = softplus(z)
            if masked:
                soft = jnp.where(key_j < key_i, soft, 0.0)
            high = soft.astype(BF16)
            low = (soft - high.astype(F32)).astype(BF16)
            after = jnp.dot(high, later, preferred_element_type=F32) + jnp.dot(low, later, preferred_element_type=F32)
            weight = jnp.exp(z - soft - after)
            if masked:
                weight = jnp.where(key_j < key_i, weight, 0.0)
            partial[slot, :, cols] = jnp.dot(weight.astype(BF16), vals, preferred_element_type=F32)
            total = after[:, 0:1] + soft[:, 0:1]
            totals[h] = jnp.where(lane == slot, total, totals[h])

    def visit_at(step, both=True):
        def side(i, carry):
            slot = ring(pos + (2 * i - 1) * step)

            @pl.when(slot < sp)
            def _():
                visit(slot, False)

            return carry

        lax.fori_loop(0, 2 if both else 1, side, 0)

    totals[...] = jnp.zeros(totals.shape, F32)
    visit(sp, True)

    def w_event(m):
        return m // 4 + 1, m % 4

    def body(s, carry):
        if n > 4:
            take("kv", s + 1, 0, True)
            take("kv", s, 1, True)
            take("w", *w_event(2 * s + 1), True)
            take("w", *w_event(2 * s + 2), True)
            visit_at(s)
        return carry

    def convolve():
        halo.wait_recv()
        ext[pl.ds(HALO, toks)] = prod_sc[...].astype(F32)
        ext[pl.ds(0, HALO)] = jnp.where(sp == 0, 0.0, prev[...].astype(F32))
        summed = jnp.zeros((toks, ext.shape[1]), F32)
        for tap in range(CONV_K):
            summed = summed + taps_ref[tap : tap + 1, :] * ext[pl.ds(HALO - (CONV_K - 1) + tap, toks)]
        ext[pl.ds(HALO, toks)] = gate_sc[...].astype(F32) * summed
        for i, g in enumerate(order):
            conv[pl.ds(i * rows, rows)] = ext[pl.ds(pl.multiple_of(HALO + g * rows, HALO), rows)].astype(BF16)

    loops = max(last - 3, 0)
    lax.fori_loop(1, 1 + loops, body, 0)
    w_done = 3 + 2 * loops
    convolve()
    for s in range(1 + loops, last + 1):
        if s + 1 <= last:
            take("kv", s + 1, 0)
        take("kv", s, 1)
        for m in range(w_done, w_done + 2 if s < last else w_done + 1):
            take("w", *w_event(m))
            w_done += 1
        visit_at(s, s < last)

    def combine(i, carry):
        slot = sp - i
        suffixes = []
        for h in range(heads):
            cols = pl.ds(h * HEAD_DIM, HEAD_DIM)
            suffix = carry[h]
            ext[pl.ds(HALO, toks), cols] += jnp.exp(-suffix) * partial[slot, :, cols]
            total = jnp.sum(jnp.where(lane == slot, totals[h], 0.0), axis=1, keepdims=True)
            suffixes.append(suffix + total)
        return tuple(suffixes)

    ext[...] = jnp.zeros(ext.shape, F32)
    suffixes = lax.fori_loop(0, sp + 1, combine, tuple(jnp.zeros((toks, 1), F32) for _ in range(heads)))
    for h in range(heads):
        spread = jnp.broadcast_to(suffixes[h], (toks, 128)).T[0:1, :]
        logw_ref[h : h + 1, :] = jnp.log(jnp.maximum(1.0 - jnp.exp(-spread), 0.05))
    for i, g in enumerate(order):
        attn[pl.ds(i * rows, rows)] = ext[pl.ds(pl.multiple_of(HALO + g * rows, HALO), rows), 0 : attn.shape[1]].astype(BF16)

    def block_of(i):
        return ring(pos - (i + 1) // 2) if i % 2 else ring(pos + i // 2)

    def d2d_copy(i):
        return push(snd.at[i], d2d.at[i], d2d_sem.at[0, i], d2d_sem.at[1, i], {"tp": near})

    def x_copy(i):
        return push(xsnd.at[i], xrcv.at[i], x_sem.at[0, i], x_sem.at[1, i], {"tp": far})

    def first(i):
        j = block_of(i)
        share = lax.dot_general(attn[...], wo[j, 0], NT, preferred_element_type=F32)
        share = (share + lax.dot_general(conv[...], wo[j, 1], NT, preferred_element_type=F32)).astype(BF16)
        snd[i] = share[2 * rows :]
        keep[i] = share[: 2 * rows]
        d2d_copy(i).start()

    def second(i):
        d2d_copy(i).wait_recv()
        xsnd[i] = (keep[i, pl.ds(rows, rows)].astype(F32) + d2d[i, pl.ds(rows, rows)].astype(F32)).astype(BF16)
        x_copy(i).start()

    def third(i):
        x_copy(i).wait_recv()
        own = keep[i, pl.ds(0, rows)].astype(F32) + d2d[i, pl.ds(0, rows)].astype(F32)
        done = (own + xrcv[i].astype(F32)).astype(BF16)
        if len(out_ref.shape) == 3:
            out_ref[block_of(i)] = done
        else:
            feats = keep.shape[2]
            out_ref[:, pl.ds(pl.multiple_of(block_of(i) * feats, feats), feats)] = done

    for i in range(n):
        while w_done < max(4 * ((i + 1) // 2), min(10 + i, 4 * last)):
            take("w", *w_event(w_done))
            w_done += 1
        first(i)
        if i >= 1:
            second(i - 1)
        if i >= 3:
            third(i - 3)
    second(n - 1)
    for i in range(max(n - 3, 0), n):
        third(i)

    for copy in (*to_far, to_near, *relay, halo):
        copy.wait_send()
    for part, sem, chunks in rings.values():
        for step in range(1, last + 1):
            for chunk in range(chunks):
                for way in ways(step, chunk, chunks):
                    hop(part, sem, way, step, chunk).wait_send()
    for i in range(n):
        d2d_copy(i).wait_send()
        x_copy(i).wait_send()


def local(
    n, tokens, norm_gain, w_query, w_key, w_value, score_shift, w_conv_b, w_conv_c, w_conv_u,
    conv_kernel, w_out_att, w_out_conv,
):
    rows, d = tokens.shape
    toks = 4 * rows
    feats, att_cols = w_out_att.shape
    conv_cols = w_out_conv.shape[1]
    heads = score_shift.shape[0]
    kv_cols = w_key.shape[1]
    vmem = pl.BlockSpec(memory_space=pltpu.VMEM)
    smem = pl.BlockSpec(memory_space=pltpu.SMEM)
    hbm = pl.BlockSpec(memory_space=pl.ANY)
    dma = pltpu.SemaphoreType.DMA
    wide = feats % 128 == 0
    out, logw = pl.pallas_call(
        functools.partial(kernel, n),
        out_shape=(
            jax.ShapeDtypeStruct((rows, n * feats) if wide else (n, rows, feats), BF16),
            jax.ShapeDtypeStruct((heads, toks), F32),
        ),
        in_specs=[vmem, vmem, hbm, hbm, hbm, smem, hbm, hbm, hbm, vmem, hbm, hbm],
        out_specs=(vmem, vmem),
        scratch_shapes=[
            *[pltpu.VMEM(w.shape, BF16) for w in (w_query, w_key, w_value, w_conv_b, w_conv_c, w_conv_u)],
            pltpu.VMEM((4, rows, d), BF16),
            pltpu.VMEM((2 * rows, d), BF16),
            pltpu.VMEM((toks, w_query.shape[1]), BF16),
            pltpu.VMEM((n, 2, 2, 2 * rows, kv_cols), BF16),
            pltpu.VMEM((n, 2, feats, att_cols), BF16),
            pltpu.VMEM((toks, conv_cols), BF16),
            pltpu.VMEM((toks, conv_cols), BF16),
            pltpu.VMEM((HALO, conv_cols), BF16),
            pltpu.VMEM((toks + HALO, max(conv_cols, att_cols)), F32),
            pltpu.VMEM((toks, att_cols), BF16),
            pltpu.VMEM((toks, conv_cols), BF16),
            pltpu.VMEM((n, toks, att_cols), F32),
            pltpu.VMEM((heads, toks, 128), F32),
            pltpu.VMEM((n, 2 * rows, feats), BF16),
            pltpu.VMEM((n, 2 * rows, feats), BF16),
            pltpu.VMEM((n, 2 * rows, feats), BF16),
            pltpu.VMEM((n, rows, feats), BF16),
            pltpu.VMEM((n, rows, feats), BF16),
            dma((8,)), dma((5,)), dma((5,)), dma((2, 2, n // 2, 2)), dma((2, 2, n // 2, 4)), dma((2,)), dma((2, n)), dma((2, n)),
        ],
        compiler_params=pltpu.CompilerParams(
            collective_id=0, has_side_effects=True, vmem_limit_bytes=60 * 1024 * 1024
        ),
    )(
        tokens, norm_gain.reshape(1, d), w_query, w_key, w_value, score_shift.reshape(1, heads),
        w_conv_b, w_conv_c, w_conv_u, conv_kernel, w_out_att, w_out_conv,
    )
    if not wide:
        out = out.transpose(1, 0, 2).reshape(rows, n * feats)
    return (out, logw.T)

def grid_kernel(
    n,
    tok_ref, gain_ref, wq_hbm, wk_hbm, wv_hbm, shift_ref, wb_hbm, wc_hbm, wu_hbm, taps_ref, woa_ref, woc_ref,
    out_ref, logw_ref,
    wq, wkv, wb, wc, wu, xall, normed, q_sc, kv, wo, gate_sc, prod_sc, prev, ext, attn, conv, acc, suffix,
    snd, keep, d2d, xsnd, xrcv, guest, gsnd, grcv,
    load_sem, tok_ssem, tok_rsem, kv_ssem, kv_fsem, kv_rsem, w_ssem, w_rsem, halo_sem, d2d_sem, x_sem,
    act_sem, ret_sem, near_by, further,
):
    sp = lax.axis_index("sp")
    t = lax.axis_index("tp")
    z = sp // 2
    y = sp % 2
    near = t + 1 - 2 * (t % 2)
    far = t + 2 - 4 * ((t // 2) % 2)
    diag = near + 2 - 4 * ((near // 2) % 2)
    up, down, side = sp + 2, sp - 2, sp + 1 - 2 * y
    ways = (up, down, side)
    host = sp + 2 - 4 * (z % 2)
    levels = n // 2
    has_up, has_down = z < levels - 1, z > 0
    outer = jnp.logical_or(z == 0, z == levels - 1)
    inner = jnp.logical_and(z > 0, z < levels - 1)
    rows = tok_ref.shape[0]
    toks = 4 * rows
    half = rows // 2
    fpart = wo.shape[2] // 2
    feats = wo.shape[2]
    heads = q_sc.shape[1] // HEAD_DIM
    kv_cols = kv.shape[4]
    grouping = heads // (kv_cols // HEAD_DIM)

    def pick(vals):
        out = vals[0]
        for i in range(1, n):
            if vals[i] != vals[0] or not isinstance(out, int):
                out = jnp.where(sp == i, vals[i], out)
        return out

    def guard(cond):
        return pl.when(cond)

    loads = [
        pltpu.make_async_copy(src, dst, load_sem.at[i])
        for i, (src, dst) in enumerate(
            (
                (wk_hbm, wkv.at[:, pl.ds(0, kv_cols)]), (wv_hbm, wkv.at[:, pl.ds(kv_cols, kv_cols)]),
                (wc_hbm, wc), (wu_hbm, wu), (wq_hbm, wq), (wb_hbm, wb),
            )
        )
    ]
    own_loads = [
        pltpu.make_async_copy(src, wo.at[sp, i], load_sem.at[6 + i]) for i, src in enumerate((woa_ref, woc_ref))
    ]
    barrier = pltpu.get_barrier_semaphore()

    def tell(sem, place):
        pl.semaphore_signal(sem, inc=1, device_id={"sp": place}, device_id_type=MESH)

    def tell_column(sem):
        guard(has_up)(lambda: tell(sem, up))
        guard(has_down)(lambda: tell(sem, down))

    column = has_up.astype(jnp.int32) + has_down.astype(jnp.int32)
    for place in (near, far):
        pl.semaphore_signal(barrier, inc=1, device_id={"tp": place}, device_id_type=MESH)
    tell(barrier, side)
    tell_column(barrier)
    for load in (*own_loads, *loads):
        load.start()
    pl.semaphore_wait(barrier, 3 + column)

    def push(src, dst, ssem, rsem, who):
        return pltpu.make_async_remote_copy(
            src_ref=src, dst_ref=dst, send_sem=ssem, recv_sem=rsem, device_id=who, device_id_type=MESH
        )

    to_far = [
        push(tok_ref.at[pl.ds(c * half, half)], xall.at[t, pl.ds(c * half, half)], tok_ssem.at[c], tok_rsem.at[c], {"tp": far})
        for c in range(2)
    ]
    to_near = push(tok_ref, xall.at[t], tok_ssem.at[2], tok_rsem.at[2], {"tp": near})
    relay = [
        push(xall.at[far, pl.ds(c * half, half)], xall.at[far, pl.ds(c * half, half)], tok_ssem.at[3 + c], tok_rsem.at[3 + c], {"tp": near})
        for c in range(2)
    ]
    for copy in to_far:
        copy.start()
    to_near.start()
    tell_column(near_by)

    def w_copy(h, c, d):
        view = wo.at[h, c // 2, pl.ds(pl.multiple_of((c % 2) * fpart, fpart), fpart)]
        return push(view, view, w_ssem.at[d, h, c], w_rsem.at[h, c], {"sp": ways[d]})

    def w_spread(vals, act):
        code = pick(vals)
        for d in range(3):
            if any(v >= 0 and v // 2**d % 2 for v in vals):
                guard(jnp.logical_and(code >= 0, code // 2**d % 2 == 1))(
                    lambda d=d: act(w_copy(code // 64, code // 8 % 8, d))
                )

    def w_own(c, act):
        mask = pick(W_OWN[c])
        for d in range(3):
            if any(v // 2**d % 2 for v in W_OWN[c]):
                guard(mask // 2**d % 2 == 1)(lambda d=d: act(w_copy(sp, c, d)))

    def pump(point):
        for vals in W_EVENTS[point]:
            code = pick(vals)

            @pl.when(code >= 0)
            def _():
                h, c = code // 64, code // 8 % 8
                w_copy(h, c, 0).wait_recv()
                for d in range(3):
                    if any(v >= 0 and v // 2**d % 2 for v in vals):
                        guard(code // 2**d % 2 == 1)(lambda d=d: w_copy(h, c, d).start())

    for load in own_loads:
        load.wait()
    for c in (0, 1):
        w_own(c, lambda copy: copy.start())

    early = t // 2

    def kv_copy(slot, part, ssem, who):
        view = kv.at[slot, early + part * (1 - 2 * early)]
        return push(view, view, ssem, kv_rsem.at[slot, part], {"sp": who})

    def kv_out(part, act):
        for step in range(levels - 1, 0, -1):
            guard(z + step < levels)(lambda step=step: act(kv_copy(sp, part, kv_ssem.at[part, step], sp + 2 * step)))
        guard(y == 0)(lambda: act(kv_copy(sp, part, kv_ssem.at[part, 0], side)))

    def kv_across(part, step, act):
        guard(z >= step)(lambda: act(kv_copy(sp - 2 * step, part, kv_fsem.at[part, step - 1], side)))

    def kv_pass(part, step):
        def both(copy):
            copy.wait_recv()
            copy.start()

        kv_across(part, step, both)

    def dot(w):
        return jnp.dot(normed[...], w[...], preferred_element_type=F32)

    def project_kv(groups, pair):
        for i, g in enumerate(groups):
            x = (tok_ref[...] if g is None else xall[g]).astype(F32)
            inverse = lax.rsqrt(jnp.mean(x * x, axis=-1, keepdims=True) + 1e-06)
            at = rows * (t % 2 if i == 0 else 1 - t % 2)
            normed[pl.ds(pl.multiple_of(at, rows), rows)] = (x * inverse * gain_ref[...]).astype(BF16)
        both = dot(wkv).astype(BF16)
        kv[sp, pair, 0] = both[:, :kv_cols]
        kv[sp, pair, 1] = both[:, kv_cols:]

    def project_rest(pair, points):
        at = pl.ds(pl.multiple_of(pair * 2 * rows, 2 * rows), 2 * rows)
        gate = dot(wc).astype(BF16).astype(F32)
        pump(points[0])
        prod_sc[at] = (gate * dot(wu).astype(BF16).astype(F32)).astype(BF16)
        pump(points[1])
        q_sc[at] = dot(wq).astype(BF16)
        pump(points[2])
        gate_sc[at] = dot(wb).astype(BF16)
        pump(points[3])

    to_near.wait_recv()
    for load in loads[:2]:
        load.wait()
    project_kv((None, near), early)
    pl.semaphore_wait(near_by, column)
    tell_column(further)
    pl.semaphore_wait(further, column)
    kv_out(0, lambda copy: copy.start())
    for c in (2, 3):
        w_own(c, lambda copy: copy.start())
    for load in loads[2:]:
        load.wait()
    pump(0)
    project_rest(early, (1, 2, 3, 4))
    to_far[0].wait_recv()
    relay[0].start()
    for step in range(1, levels):
        kv_pass(0, step)
    pump(5)
    to_far[1].wait_recv()
    relay[1].start()
    for c in range(2):
        relay[c].wait_recv()
    project_kv((far, diag), 1 - early)
    kv_out(1, lambda copy: copy.start())
    pump(6)
    project_rest(1 - early, (7, 8, 9, 10))
    halo = push(prod_sc.at[pl.ds(toks - HALO, HALO)], prev, halo_sem.at[0], halo_sem.at[1], {"sp": sp + 1})
    guard(sp < n - 1)(halo.start)

    key_i = lax.broadcasted_iota(jnp.int32, (toks, toks), 0)
    key_j = lax.broadcasted_iota(jnp.int32, (toks, toks), 1)
    later = (key_i > key_j).astype(F32).astype(BF16)
    scale = HEAD_DIM ** (-0.5)
    order = (t, far, near, diag)

    def visit(slot, masked):
        for h in range(heads):
            cols = pl.ds(h * HEAD_DIM, HEAD_DIM)
            kv_at = pl.ds((h // grouping) * HEAD_DIM, HEAD_DIM)
            keys = kv[slot, :, 0, :, kv_at].reshape(toks, HEAD_DIM)
            vals = kv[slot, :, 1, :, kv_at].reshape(toks, HEAD_DIM)
            s = lax.dot_general(q_sc[:, cols], keys, NT, preferred_element_type=F32) * scale + shift_ref[0, h]
            soft = softplus(s)
            if masked:
                soft = jnp.where(key_j < key_i, soft, 0.0)
            high = soft.astype(BF16)
            low = (soft - high.astype(F32)).astype(BF16)
            after = jnp.dot(high, later, preferred_element_type=F32) + jnp.dot(low, later, preferred_element_type=F32)
            weight = jnp.exp(s - soft - after)
            if masked:
                weight = jnp.where(key_j < key_i, weight, 0.0)
            part = jnp.dot(weight.astype(BF16), vals, preferred_element_type=F32)
            total = jnp.broadcast_to(after[:, 0:1] + soft[:, 0:1], (toks, HEAD_DIM))
            if masked:
                acc[:, cols] = part
                suffix[h] = total
            else:
                acc[:, cols] += jnp.exp(-suffix[h]) * part
                suffix[h] += total

    def convolve():
        @pl.when(sp == 0)
        def _():
            prev[...] = jnp.zeros(prev.shape, BF16)

        guard(sp > 0)(halo.wait_recv)
        ext[pl.ds(HALO, toks)] = prod_sc[...].astype(F32)
        ext[pl.ds(0, HALO)] = prev[...].astype(F32)
        summed = jnp.zeros((toks, ext.shape[1]), F32)
        for tap in range(CONV_K):
            summed = summed + taps_ref[tap : tap + 1, :] * ext[pl.ds(HALO - (CONV_K - 1) + tap, toks)]
        ext[pl.ds(HALO, toks)] = gate_sc[...].astype(F32) * summed
        for i, g in enumerate(order):
            conv[pl.ds(i * rows, rows)] = ext[pl.ds(pl.multiple_of(HALO + g * rows, HALO), rows)].astype(BF16)

    def act_copy(i):
        return push((attn, conv)[i], guest.at[i], act_sem.at[0, i], act_sem.at[1, i], {"sp": host})

    for step in range(1, levels):
        kv_pass(1, step)
    visit(sp, True)
    pump(11)
    convolve()
    guard(outer)(lambda: act_copy(1).start())
    pump(12)
    for i in range(1, n):
        slot = sp - i

        @pl.when(slot >= 0)
        def _():
            def take(part):
                kv_copy(slot, part, kv_ssem.at[part, 0], side).wait_recv()

            if i % 2 == 1:
                take(0)
                take(1)
            visit(slot, False)

        pump(12 + i)

    for h in range(heads):
        spread = suffix[h].T[0:1, :]
        logw_ref[h : h + 1, :] = jnp.log(jnp.maximum(1.0 - jnp.exp(-spread), 0.05))
    for i, g in enumerate(order):
        attn[pl.ds(i * rows, rows)] = acc[pl.ds(pl.multiple_of(g * rows, rows), rows)].astype(BF16)
    guard(outer)(lambda: act_copy(0).start())

    def d2d_copy(i):
        return push(snd.at[i], d2d.at[i], d2d_sem.at[0, i], d2d_sem.at[1, i], {"tp": near})

    def x_copy(i):
        return push(xsnd.at[i], xrcv.at[i], x_sem.at[0, i], x_sem.at[1, i], {"tp": far})

    def ret_copy(r):
        return push(gsnd.at[r], grcv.at[r], ret_sem.at[0, r], ret_sem.at[1, r], {"sp": host})

    def put(h, block):
        out_ref[:, pl.ds(pl.multiple_of(h * feats, feats), feats)] = block

    def active(i):
        vals = CELLS[i]
        if all(v >= 0 for v in vals):
            return lambda body: body()
        return pl.when(pick(vals) >= 0)

    own_cells = n

    def first(i):
        @active(i)
        def _():
            j = pick(CELLS[i])
            a, b = (attn, conv) if i < own_cells else (guest.at[0], guest.at[1])
            share = lax.dot_general(a[...], wo[j, 0], NT, preferred_element_type=F32)
            share = (share + lax.dot_general(b[...], wo[j, 1], NT, preferred_element_type=F32)).astype(BF16)
            snd[i] = share[2 * rows :]
            keep[i] = share[: 2 * rows]
            d2d_copy(i).start()

    def second(i):
        @active(i)
        def _():
            d2d_copy(i).wait_recv()
            xsnd[i] = (keep[i, pl.ds(rows, rows)].astype(F32) + d2d[i, pl.ds(rows, rows)].astype(F32)).astype(BF16)
            x_copy(i).start()

    def third(i):
        @active(i)
        def _():
            x_copy(i).wait_recv()
            own = keep[i, pl.ds(0, rows)].astype(F32) + d2d[i, pl.ds(0, rows)].astype(F32)
            done = (own + xrcv[i].astype(F32)).astype(BF16)
            if i < own_cells:
                put(pick(CELLS[i]), done)
            else:
                gsnd[i - own_cells] = done
                ret_copy(i - own_cells).start()

    done_first = []
    for step, i in enumerate(CELL_ORDER):
        pump(20 + step)
        if i == own_cells:
            @pl.when(inner)
            def _():
                act_copy(1).wait_recv()
                act_copy(0).wait_recv()

        first(i)
        done_first.append(i)
        if step >= 1:
            second(done_first[step - 1])
        if step >= 3:
            third(done_first[step - 3])
    second(done_first[-1])
    for i in done_first[-3:]:
        third(i)
    for r in range(len(CELLS) - own_cells):
        @pl.when(outer)
        def _():
            ret_copy(r).wait_recv()
            put(pick(CELL_BACK[r]), grcv[r])

    for copy in (*to_far, to_near, *relay):
        copy.wait_send()
    guard(sp < n - 1)(halo.wait_send)
    for part in range(2):
        kv_out(part, lambda copy: copy.wait_send())
        for step in range(1, levels):
            kv_across(part, step, lambda copy: copy.wait_send())
    for c in range(4):
        w_own(c, lambda copy: copy.wait_send())
    for slots in W_EVENTS:
        for vals in slots:
            w_spread(vals, lambda copy: copy.wait_send())

    @pl.when(outer)
    def _():
        for i in range(2):
            act_copy(i).wait_send()

    for i in range(len(CELLS)):
        @active(i)
        def _():
            d2d_copy(i).wait_send()
            x_copy(i).wait_send()
            if i >= own_cells:
                ret_copy(i - own_cells).wait_send()


def grid_local(
    n, tokens, norm_gain, w_query, w_key, w_value, score_shift, w_conv_b, w_conv_c, w_conv_u,
    conv_kernel, w_out_att, w_out_conv,
):
    rows, d = tokens.shape
    toks = 4 * rows
    feats, att_cols = w_out_att.shape
    conv_cols = w_out_conv.shape[1]
    heads = score_shift.shape[0]
    kv_cols = w_key.shape[1]
    cells = len(CELLS)
    guests = cells - n
    vmem = pl.BlockSpec(memory_space=pltpu.VMEM)
    smem = pl.BlockSpec(memory_space=pltpu.SMEM)
    hbm = pl.BlockSpec(memory_space=pl.ANY)
    dma = pltpu.SemaphoreType.DMA
    regular = pltpu.SemaphoreType.REGULAR
    out, logw = pl.pallas_call(
        functools.partial(grid_kernel, n),
        out_shape=(
            jax.ShapeDtypeStruct((rows, n * feats), BF16),
            jax.ShapeDtypeStruct((heads, toks), F32),
        ),
        in_specs=[vmem, vmem, hbm, hbm, hbm, smem, hbm, hbm, hbm, vmem, hbm, hbm],
        out_specs=(vmem, vmem),
        scratch_shapes=[
            pltpu.VMEM(w_query.shape, BF16),
            pltpu.VMEM((d, 2 * kv_cols), BF16),
            *[pltpu.VMEM(w.shape, BF16) for w in (w_conv_b, w_conv_c, w_conv_u)],
            pltpu.VMEM((4, rows, d), BF16),
            pltpu.VMEM((2 * rows, d), BF16),
            pltpu.VMEM((toks, w_query.shape[1]), BF16),
            pltpu.VMEM((n, 2, 2, 2 * rows, kv_cols), BF16),
            pltpu.VMEM((n, 2, feats, att_cols), BF16),
            pltpu.VMEM((toks, conv_cols), BF16),
            pltpu.VMEM((toks, conv_cols), BF16),
            pltpu.VMEM((HALO, conv_cols), BF16),
            pltpu.VMEM((toks + HALO, conv_cols), F32),
            pltpu.VMEM((toks, att_cols), BF16),
            pltpu.VMEM((toks, conv_cols), BF16),
            pltpu.VMEM((toks, att_cols), F32),
            pltpu.VMEM((heads, toks, HEAD_DIM), F32),
            *[pltpu.VMEM((cells, 2 * rows, feats), BF16)] * 3,
            *[pltpu.VMEM((cells, rows, feats), BF16)] * 2,
            pltpu.VMEM((2, toks, att_cols), BF16),
            *[pltpu.VMEM((guests, rows, feats), BF16)] * 2,
            dma((8,)), dma((5,)), dma((5,)), dma((2, n // 2)), dma((2, n // 2 - 1)), dma((n, 2)), dma((3, n, 4)), dma((n, 4)),
            dma((2,)), dma((2, cells)), dma((2, cells)), dma((2, 2)), dma((2, guests)), regular, regular,
        ],
        compiler_params=pltpu.CompilerParams(
            collective_id=0, has_side_effects=True, vmem_limit_bytes=60 * 1024 * 1024
        ),
    )(
        tokens, norm_gain.reshape(1, d), w_query, w_key, w_value, score_shift.reshape(1, heads),
        w_conv_b, w_conv_c, w_conv_u, conv_kernel, w_out_att, w_out_conv,
    )
    return (out, logw.T)


def solution(mesh):
    n = mesh.shape["sp"]
    body = grid_local if n == len(W_OWN[0]) and mesh.shape["tp"] == 4 else local
    return jax.shard_map(
        functools.partial(body, n),
        mesh=mesh,
        in_specs=(
            P(("sp", "tp"), None), P(), P(None, "tp"), P(None, "tp"), P(None, "tp"), P("tp"),
            P(None, "tp"), P(None, "tp"), P(None, "tp"), P(None, "tp"), P("sp", "tp"), P("sp", "tp"),
        ),
        out_specs=(P(("sp", "tp"), None), P("sp", "tp")),
        check_vma=False,
    )
```

```python
import functools

import jax
import jax.numpy as jnp
from jax import lax
from jax.experimental import pallas as pl
from jax.experimental.pallas import tpu as pltpu
from jax.sharding import PartitionSpec as P

HEAD_DIM = 128
CONV_K = 3
HALO = 16
F32 = jnp.float32
BF16 = jnp.bfloat16
MESH = pl.DeviceIdType.MESH
NT = (((1,), (1,)), ((), ()))
EVENTS = [[(10, 138, 270, 398, 526, 646, 780, 908), (-1, -1, -1, -1, -1, 664, -1, -1)],
 [(74, 194, 330, 450, 586, 706, 840, 924),
  (26, 154, 278, 414, 542, 662, 796, -1),
  (-1, -1, 296, -1, -1, 680, -1, -1)],
 [],
 [(-1, 168, 292, 428, 548, 692, 804, 940)],
 [(-1, -1, -1, -1, -1, 393, -1, -1)],
 [(42, 162, 290, 418, 554, 674, 808, -1), (-1, -1, 312, -1, -1, -1, -1, -1)],
 [(-1, 184, 75, 203, 331, 459, 585, 713), (-1, -1, 308, 436, 564, 517, 820, 948)],
 [(58, 178, 306, 440, 562, 409, 824, 952),
  (-1, 393, 517, 434, 265, 690, 901, 773),
  (-1, -1, 553, 645, 773, 901, -1, 649)],
 [(90, 210, 346, 466, 75, 203, 329, 457),
  (131, 3, 405, 648, 602, 722, 856, 789),
  (265, 425, -1, 661, 677, 917, 917, -1)],
 [],
 [(-1, 441, 533, 293, 789, 933, 537, 665), (-1, -1, -1, -1, -1, 425, 933, 805)],
 [(147, 19, 3, 131, -1, -1, -1, -1), (281, -1, -1, -1, -1, -1, -1, -1)],
 [(-1, -1, 569, 664, -1, -1, -1, -1)],
 [(-1, -1, 91, 219, 347, 475, 73, 201)],
 [(313, 649, 19, 147, 805, 773, -1, -1), (-1, -1, 548, 693, -1, -1, -1, -1)],
 [(-1, 65, 57, 321, 258, 577, 601, 729),
  (-1, 81, 35, 337, 281, 593, 345, 833),
  (-1, -1, 564, -1, 821, -1, 949, 849),
  (-1, -1, 681, -1, 449, -1, 553, -1),
  (-1, -1, 193, -1, 465, -1, 645, -1),
  (-1, -1, 209, -1, -1, -1, 705, -1),
  (-1, -1, -1, -1, -1, -1, 721, -1)],
 [(-1, -1, 676, 696, 91, 386, 569, -1), (-1, -1, -1, -1, 274, 441, -1, -1), (-1, -1, -1, -1, 297, -1, -1, -1)],
 [(-1, -1, -1, 517, 917, 789, 89, 473),
  (-1, -1, -1, 163, 290, 321, 449, 821),
  (-1, -1, -1, 905, 313, 337, 465, 681),
  (-1, -1, -1, 65, 193, -1, -1, 577),
  (-1, -1, -1, 81, 209, -1, -1, 593)],
 [(-1, -1, -1, -1, -1, 219, -1, 697), (-1, -1, -1, -1, -1, 514, -1, -1), (-1, -1, -1, -1, -1, 137, -1, -1)],
 [(-1, -1, -1, -1, -1, 805, 297, 217),
  (-1, -1, -1, -1, -1, 402, 193, 321),
  (-1, -1, -1, -1, -1, 65, 209, 337),
  (-1, -1, -1, -1, -1, 81, -1, -1)],
 [],
 [(-1, -1, -1, -1, -1, -1, -1, 393),
  (-1, -1, -1, -1, -1, -1, -1, 565),
  (-1, -1, -1, -1, -1, -1, -1, 65),
  (-1, -1, -1, -1, -1, -1, -1, 81)],
 [(-1, -1, 50, 179, 403, 277, -1, 425), (-1, -1, -1, 549, 9, -1, -1, -1), (-1, -1, -1, -1, 949, -1, -1, -1)],
 [(161, 401, -1, 937, -1, 418, -1, -1), (177, -1, -1, -1, -1, 169, -1, -1), (-1, -1, -1, -1, -1, 945, -1, -1)],
 [(289, 665, 147, 19, -1, -1, 313, -1), (-1, 33, -1, 673, -1, -1, 513, -1), (-1, 49, -1, -1, -1, -1, -1, -1)],
 [(385, 34, 825, 35, 306, 817, 657, 513),
  (401, 697, 385, 1, 385, -1, 673, 529),
  (417, 257, 417, 49, 417, -1, 689, 545),
  (433, 273, 433, -1, 433, -1, -1, -1),
  (-1, 289, -1, -1, -1, -1, -1, -1),
  (-1, 305, -1, -1, -1, -1, -1, -1)],
 [(162, 531, 691, 769, 434, 259, 441, 257),
  (537, 513, 769, 785, 57, 185, 257, 273),
  (178, 545, 785, 801, 897, 145, 273, 289),
  (569, 561, 801, 817, 929, -1, -1, 305),
  (513, -1, -1, -1, -1, -1, -1, -1),
  (545, -1, -1, -1, -1, -1, -1, -1)],
 [(681, 673, 641, -1, 17, 274, 385, 401),
  (641, -1, 657, -1, 33, 289, 401, 433),
  (657, -1, -1, -1, -1, 305, 417, -1),
  (689, -1, -1, -1, -1, -1, -1, -1)],
 [(-1, -1, 953, 257, 641, 529, -1, -1),
  (-1, -1, 897, 273, 657, 545, -1, -1),
  (-1, -1, 913, 305, 689, 561, -1, -1),
  (-1, -1, 929, -1, -1, -1, -1, -1)],
 [(-1, -1, -1, 529, 129, 1, -1, -1),
  (-1, -1, -1, 561, 145, 17, -1, -1),
  (-1, -1, -1, -1, 161, 33, -1, -1),
  (-1, -1, -1, -1, 177, 49, -1, -1)],
 [(-1, -1, -1, 913, -1, -1, -1, -1), (-1, -1, -1, 945, -1, -1, -1, -1)],
 [(-1, -1, 129, -1, -1, -1, -1, -1), (-1, -1, 161, -1, -1, -1, -1, -1), (-1, -1, 177, -1, -1, -1, -1, -1)],
 []]
CELLS = [(0, 1, 2, 3, 4, 5, 6, 7),
 (1, 3, 4, 1, 6, 7, 7, 5),
 (2, 0, 0, 5, 2, 3, 4, 6),
 (3, 2, 3, 0, 3, 6, 5, 4),
 (4, 4, 14, 14, 7, 1, 2, 2),
 (5, 5, 5, 6, 0, 2, 3, 3),
 (-1, -1, 23, 2, 5, 4, -1, -1),
 (-1, -1, 6, 4, 1, 0, -1, -1),
 (-1, -1, 7, 23, 8, 8, -1, -1),
 (-1, -1, 1, 7, 17, 17, -1, -1)]
CELL_BACK = [(6, 6, -1, -1, -1, -1, 0, 0), (7, 7, -1, -1, -1, -1, 1, 1)]


def softplus(z):
    u = jnp.exp(-jnp.abs(z))
    small = u * (1.0 - u * (0.5 - u * (1.0 / 3.0 - u * 0.25)))
    return jnp.maximum(z, 0.0) + jnp.where(u < 0.01, small, jnp.log(1.0 + u))


def kernel(
    n,
    tok_ref, gain_ref, wq_hbm, wk_hbm, wv_hbm, shift_ref, wb_hbm, wc_hbm, wu_hbm, taps_ref, woa_ref, woc_ref,
    out_ref, logw_ref,
    wq, wk, wv, wb, wc, wu, xall, normed, q_sc, kv, wo, gate_sc, prod_sc, prev, ext, attn, conv, partial, totals,
    snd, keep, d2d, xsnd, xrcv,
    load_sem, tok_ssem, tok_rsem, kv_sem, w_sem, halo_sem, d2d_sem, x_sem,
):
    sp = lax.axis_index("sp")
    t = lax.axis_index("tp")
    near = t + 1 - 2 * (t % 2)
    far = t + 2 - 4 * ((t // 2) % 2)
    diag = near + 2 - 4 * ((near // 2) % 2)
    pos = jnp.where(sp % 2 == 0, sp // 2, n - 1 - sp // 2)

    def ring(place):
        place = (place + 2 * n) % n
        return jnp.where(place < n // 2, 2 * place, 2 * (n - 1 - place) + 1)

    right, left = ring(pos + 1), ring(pos - 1)
    following, leading = (sp + 1) % n, (sp + n - 1) % n
    rows = tok_ref.shape[0]
    toks = 4 * rows
    half = rows // 2
    fpart = wo.shape[2] // 2
    heads = q_sc.shape[1] // HEAD_DIM
    kv_cols = kv.shape[4]
    grouping = heads // (kv_cols // HEAD_DIM)

    loads = [
        pltpu.make_async_copy(src, dst, load_sem.at[i])
        for i, (src, dst) in enumerate(
            ((wk_hbm, wk), (wv_hbm, wv), (wq_hbm, wq), (wc_hbm, wc), (wu_hbm, wu), (wb_hbm, wb))
        )
    ]
    own_loads = [
        pltpu.make_async_copy(src, wo.at[sp, i], load_sem.at[6 + i]) for i, src in enumerate((woa_ref, woc_ref))
    ]
    barrier = pltpu.get_barrier_semaphore()
    for place in (right, left, following, leading):
        pl.semaphore_signal(barrier, inc=1, device_id={"sp": place}, device_id_type=MESH)
    for place in (near, far):
        pl.semaphore_signal(barrier, inc=1, device_id={"tp": place}, device_id_type=MESH)
    for load in (*own_loads, *loads):
        load.start()
    pl.semaphore_wait(barrier, 6)

    def push(src, dst, ssem, rsem, who):
        return pltpu.make_async_remote_copy(
            src_ref=src, dst_ref=dst, send_sem=ssem, recv_sem=rsem, device_id=who, device_id_type=MESH
        )

    to_far = [
        push(tok_ref.at[pl.ds(c * half, half)], xall.at[t, pl.ds(c * half, half)], tok_ssem.at[c], tok_rsem.at[c], {"tp": far})
        for c in range(2)
    ]
    to_near = push(tok_ref, xall.at[t], tok_ssem.at[2], tok_rsem.at[2], {"tp": near})
    relay = [
        push(xall.at[far, pl.ds(c * half, half)], xall.at[far, pl.ds(c * half, half)], tok_ssem.at[3 + c], tok_rsem.at[3 + c], {"tp": near})
        for c in range(2)
    ]
    for copy in to_far:
        copy.start()
    to_near.start()

    last = n // 2

    def hop(part, sem, way, step, chunk):
        block = ring(pos - (step - 1)) if way == 0 else ring(pos + (step - 1))
        view = part(block, chunk, step)
        return push(
            view[0], view[1], sem.at[0, way, step - 1, chunk], sem.at[1, way, step - 1, chunk],
            {"sp": right if way == 0 else left},
        )

    def ways(step, chunk, chunks):
        if isinstance(step, int) and step == last:
            return (0,) if chunk < chunks // 2 else (1,)
        return (0, 1)

    early = t // 2

    def kv_part(block, chunk, step):
        view = kv.at[block, early + chunk * (1 - 2 * early)]
        return view, view

    def w_part(block, chunk, step):
        view = wo.at[block, chunk // 2, pl.ds(pl.multiple_of((chunk % 2) * fpart, fpart), fpart)]
        return view, view

    rings = {"kv": (kv_part, kv_sem, 2), "w": (w_part, w_sem, 4)}

    def emit(name, step, chunk):
        part, sem, chunks = rings[name]
        for way in ways(step, chunk, chunks):
            hop(part, sem, way, step, chunk).start()

    def take(name, step, chunk, onward=None):
        part, sem, chunks = rings[name]
        for way in ways(step, chunk, chunks):
            hop(part, sem, way, step, chunk).wait_recv()
        if onward or (onward is None and step < last):
            emit(name, step + 1, chunk)

    for load in own_loads:
        load.wait()
    for chunk in (0, 1):
        emit("w", 1, chunk)

    def dot(w):
        return jnp.dot(normed[...], w[...], preferred_element_type=F32).astype(BF16)

    def project_kv(groups, pair):
        for i, g in enumerate(groups):
            x = (tok_ref[...] if g is None else xall[g]).astype(F32)
            inverse = lax.rsqrt(jnp.mean(x * x, axis=-1, keepdims=True) + 1e-06)
            at = rows * (t % 2 if i == 0 else 1 - t % 2)
            normed[pl.ds(pl.multiple_of(at, rows), rows)] = (x * inverse * gain_ref[...]).astype(BF16)
        kv[sp, pair, 0] = dot(wk)
        kv[sp, pair, 1] = dot(wv)

    def project_rest(pair):
        at = pl.ds(pl.multiple_of(pair * 2 * rows, 2 * rows), 2 * rows)
        prod_sc[at] = (dot(wc).astype(F32) * dot(wu).astype(F32)).astype(BF16)
        q_sc[at] = dot(wq)
        gate_sc[at] = dot(wb)

    to_near.wait_recv()
    for load in loads[:2]:
        load.wait()
    project_kv((None, near), early)
    emit("kv", 1, 0)
    for chunk in (2, 3):
        emit("w", 1, chunk)
    for load in loads[2:]:
        load.wait()
    project_rest(early)
    to_far[0].wait_recv()
    relay[0].start()
    take("kv", 1, 0)
    take("w", 1, 0)
    to_far[1].wait_recv()
    relay[1].start()
    for c in range(2):
        relay[c].wait_recv()
    project_kv((far, diag), 1 - early)
    emit("kv", 1, 1)
    take("w", 1, 1)
    take("w", 1, 2)
    project_rest(1 - early)
    halo = push(prod_sc.at[pl.ds(toks - HALO, HALO)], prev, halo_sem.at[0], halo_sem.at[1], {"sp": following})
    halo.start()

    key_i = lax.broadcasted_iota(jnp.int32, (toks, toks), 0)
    key_j = lax.broadcasted_iota(jnp.int32, (toks, toks), 1)
    later = (key_i > key_j).astype(F32).astype(BF16)
    lane = lax.broadcasted_iota(jnp.int32, (toks, totals.shape[2]), 1)
    scale = HEAD_DIM ** (-0.5)
    order = (t, far, near, diag)

    def visit(slot, masked):
        for h in range(heads):
            cols = pl.ds(h * HEAD_DIM, HEAD_DIM)
            kv_at = pl.ds((h // grouping) * HEAD_DIM, HEAD_DIM)
            keys = kv[slot, :, 0, :, kv_at].reshape(toks, HEAD_DIM)
            vals = kv[slot, :, 1, :, kv_at].reshape(toks, HEAD_DIM)
            z = lax.dot_general(q_sc[:, cols], keys, NT, preferred_element_type=F32) * scale + shift_ref[0, h]
            soft = softplus(z)
            if masked:
                soft = jnp.where(key_j < key_i, soft, 0.0)
            high = soft.astype(BF16)
            low = (soft - high.astype(F32)).astype(BF16)
            after = jnp.dot(high, later, preferred_element_type=F32) + jnp.dot(low, later, preferred_element_type=F32)
            weight = jnp.exp(z - soft - after)
            if masked:
                weight = jnp.where(key_j < key_i, weight, 0.0)
            partial[slot, :, cols] = jnp.dot(weight.astype(BF16), vals, preferred_element_type=F32)
            total = after[:, 0:1] + soft[:, 0:1]
            totals[h] = jnp.where(lane == slot, total, totals[h])

    def visit_at(step, both=True):
        def side(i, carry):
            slot = ring(pos + (2 * i - 1) * step)

            @pl.when(slot < sp)
            def _():
                visit(slot, False)

            return carry

        lax.fori_loop(0, 2 if both else 1, side, 0)

    totals[...] = jnp.zeros(totals.shape, F32)
    visit(sp, True)

    def w_event(m):
        return m // 4 + 1, m % 4

    def body(s, carry):
        if n > 4:
            take("kv", s + 1, 0, True)
            take("kv", s, 1, True)
            take("w", *w_event(2 * s + 1), True)
            take("w", *w_event(2 * s + 2), True)
            visit_at(s)
        return carry

    def convolve():
        halo.wait_recv()
        ext[pl.ds(HALO, toks)] = prod_sc[...].astype(F32)
        ext[pl.ds(0, HALO)] = jnp.where(sp == 0, 0.0, prev[...].astype(F32))
        summed = jnp.zeros((toks, ext.shape[1]), F32)
        for tap in range(CONV_K):
            summed = summed + taps_ref[tap : tap + 1, :] * ext[pl.ds(HALO - (CONV_K - 1) + tap, toks)]
        ext[pl.ds(HALO, toks)] = gate_sc[...].astype(F32) * summed
        for i, g in enumerate(order):
            conv[pl.ds(i * rows, rows)] = ext[pl.ds(pl.multiple_of(HALO + g * rows, HALO), rows)].astype(BF16)

    loops = max(last - 3, 0)
    lax.fori_loop(1, 1 + loops, body, 0)
    w_done = 3 + 2 * loops
    convolve()
    for s in range(1 + loops, last + 1):
        if s + 1 <= last:
            take("kv", s + 1, 0)
        take("kv", s, 1)
        for m in range(w_done, w_done + 2 if s < last else w_done + 1):
            take("w", *w_event(m))
            w_done += 1
        visit_at(s, s < last)

    def combine(i, carry):
        slot = sp - i
        suffixes = []
        for h in range(heads):
            cols = pl.ds(h * HEAD_DIM, HEAD_DIM)
            suffix = carry[h]
            ext[pl.ds(HALO, toks), cols] += jnp.exp(-suffix) * partial[slot, :, cols]
            total = jnp.sum(jnp.where(lane == slot, totals[h], 0.0), axis=1, keepdims=True)
            suffixes.append(suffix + total)
        return tuple(suffixes)

    ext[...] = jnp.zeros(ext.shape, F32)
    suffixes = lax.fori_loop(0, sp + 1, combine, tuple(jnp.zeros((toks, 1), F32) for _ in range(heads)))
    for h in range(heads):
        spread = jnp.broadcast_to(suffixes[h], (toks, 128)).T[0:1, :]
        logw_ref[h : h + 1, :] = jnp.log(jnp.maximum(1.0 - jnp.exp(-spread), 0.05))
    for i, g in enumerate(order):
        attn[pl.ds(i * rows, rows)] = ext[pl.ds(pl.multiple_of(HALO + g * rows, HALO), rows), 0 : attn.shape[1]].astype(BF16)

    def block_of(i):
        return ring(pos - (i + 1) // 2) if i % 2 else ring(pos + i // 2)

    def d2d_copy(i):
        return push(snd.at[i], d2d.at[i], d2d_sem.at[0, i], d2d_sem.at[1, i], {"tp": near})

    def x_copy(i):
        return push(xsnd.at[i], xrcv.at[i], x_sem.at[0, i], x_sem.at[1, i], {"tp": far})

    def first(i):
        j = block_of(i)
        share = lax.dot_general(attn[...], wo[j, 0], NT, preferred_element_type=F32)
        share = (share + lax.dot_general(conv[...], wo[j, 1], NT, preferred_element_type=F32)).astype(BF16)
        snd[i] = share[2 * rows :]
        keep[i] = share[: 2 * rows]
        d2d_copy(i).start()

    def second(i):
        d2d_copy(i).wait_recv()
        xsnd[i] = (keep[i, pl.ds(rows, rows)].astype(F32) + d2d[i, pl.ds(rows, rows)].astype(F32)).astype(BF16)
        x_copy(i).start()

    def third(i):
        x_copy(i).wait_recv()
        own = keep[i, pl.ds(0, rows)].astype(F32) + d2d[i, pl.ds(0, rows)].astype(F32)
        done = (own + xrcv[i].astype(F32)).astype(BF16)
        if len(out_ref.shape) == 3:
            out_ref[block_of(i)] = done
        else:
            feats = keep.shape[2]
            out_ref[:, pl.ds(pl.multiple_of(block_of(i) * feats, feats), feats)] = done

    for i in range(n):
        while w_done < max(4 * ((i + 1) // 2), min(10 + i, 4 * last)):
            take("w", *w_event(w_done))
            w_done += 1
        first(i)
        if i >= 1:
            second(i - 1)
        if i >= 3:
            third(i - 3)
    second(n - 1)
    for i in range(max(n - 3, 0), n):
        third(i)

    for copy in (*to_far, to_near, *relay, halo):
        copy.wait_send()
    for part, sem, chunks in rings.values():
        for step in range(1, last + 1):
            for chunk in range(chunks):
                for way in ways(step, chunk, chunks):
                    hop(part, sem, way, step, chunk).wait_send()
    for i in range(n):
        d2d_copy(i).wait_send()
        x_copy(i).wait_send()


def local(
    n, tokens, norm_gain, w_query, w_key, w_value, score_shift, w_conv_b, w_conv_c, w_conv_u,
    conv_kernel, w_out_att, w_out_conv,
):
    rows, d = tokens.shape
    toks = 4 * rows
    feats, att_cols = w_out_att.shape
    conv_cols = w_out_conv.shape[1]
    heads = score_shift.shape[0]
    kv_cols = w_key.shape[1]
    vmem = pl.BlockSpec(memory_space=pltpu.VMEM)
    smem = pl.BlockSpec(memory_space=pltpu.SMEM)
    hbm = pl.BlockSpec(memory_space=pl.ANY)
    dma = pltpu.SemaphoreType.DMA
    wide = feats % 128 == 0
    out, logw = pl.pallas_call(
        functools.partial(kernel, n),
        out_shape=(
            jax.ShapeDtypeStruct((rows, n * feats) if wide else (n, rows, feats), BF16),
            jax.ShapeDtypeStruct((heads, toks), F32),
        ),
        in_specs=[vmem, vmem, hbm, hbm, hbm, smem, hbm, hbm, hbm, vmem, hbm, hbm],
        out_specs=(vmem, vmem),
        scratch_shapes=[
            *[pltpu.VMEM(w.shape, BF16) for w in (w_query, w_key, w_value, w_conv_b, w_conv_c, w_conv_u)],
            pltpu.VMEM((4, rows, d), BF16),
            pltpu.VMEM((2 * rows, d), BF16),
            pltpu.VMEM((toks, w_query.shape[1]), BF16),
            pltpu.VMEM((n, 2, 2, 2 * rows, kv_cols), BF16),
            pltpu.VMEM((n, 2, feats, att_cols), BF16),
            pltpu.VMEM((toks, conv_cols), BF16),
            pltpu.VMEM((toks, conv_cols), BF16),
            pltpu.VMEM((HALO, conv_cols), BF16),
            pltpu.VMEM((toks + HALO, max(conv_cols, att_cols)), F32),
            pltpu.VMEM((toks, att_cols), BF16),
            pltpu.VMEM((toks, conv_cols), BF16),
            pltpu.VMEM((n, toks, att_cols), F32),
            pltpu.VMEM((heads, toks, 128), F32),
            pltpu.VMEM((n, 2 * rows, feats), BF16),
            pltpu.VMEM((n, 2 * rows, feats), BF16),
            pltpu.VMEM((n, 2 * rows, feats), BF16),
            pltpu.VMEM((n, rows, feats), BF16),
            pltpu.VMEM((n, rows, feats), BF16),
            dma((8,)), dma((5,)), dma((5,)), dma((2, 2, n // 2, 2)), dma((2, 2, n // 2, 4)), dma((2,)), dma((2, n)), dma((2, n)),
        ],
        compiler_params=pltpu.CompilerParams(
            collective_id=0, has_side_effects=True, vmem_limit_bytes=60 * 1024 * 1024
        ),
    )(
        tokens, norm_gain.reshape(1, d), w_query, w_key, w_value, score_shift.reshape(1, heads),
        w_conv_b, w_conv_c, w_conv_u, conv_kernel, w_out_att, w_out_conv,
    )
    if not wide:
        out = out.transpose(1, 0, 2).reshape(rows, n * feats)
    return (out, logw.T)

def grid_kernel(
    n,
    tok_ref, gain_ref, wq_hbm, wk_hbm, wv_hbm, shift_ref, wb_hbm, wc_hbm, wu_hbm, taps_ref, woa_ref, woc_ref,
    out_ref, logw_ref,
    wq, wkv, wb, wc, wu, xall, normed, q_sc, kv, wo, gate_sc, prod_sc, prev, ext, acts, acc, suffix,
    snd, keep, d2d, xsnd, xrcv, gsnd, grcv,
    load_sem, tok_ssem, tok_rsem, kv_ssem, kv_rsem, w_ssem, w_rsem, halo_sem, d2d_sem, x_sem,
    act_sem, ret_sem, near_by,
):
    sp = lax.axis_index("sp")
    t = lax.axis_index("tp")
    z = sp // 2
    y = sp % 2
    near = t + 1 - 2 * (t % 2)
    far = t + 2 - 4 * ((t // 2) % 2)
    diag = near + 2 - 4 * ((near // 2) % 2)
    up, down, side = sp + 2, sp - 2, sp + 1 - 2 * y
    ways = (up, down, side)
    host = sp + 2 - 4 * (z % 2)
    levels = n // 2
    has_up, has_down = z < levels - 1, z > 0
    outer = jnp.logical_or(z == 0, z == levels - 1)
    rows = tok_ref.shape[0]
    toks = 4 * rows
    half = rows // 2
    fpart = wo.shape[2] // 2
    feats = wo.shape[2]
    heads = q_sc.shape[1] // HEAD_DIM
    kv_cols = kv.shape[4]
    grouping = heads // (kv_cols // HEAD_DIM)

    def pick(vals):
        out = vals[0]
        for i in range(1, n):
            if vals[i] != vals[0] or not isinstance(out, int):
                out = jnp.where(sp == i, vals[i], out)
        return out

    def guard(cond):
        return pl.when(cond)

    loads = [
        pltpu.make_async_copy(src, dst, load_sem.at[i])
        for i, (src, dst) in enumerate(
            (
                (wk_hbm, wkv.at[:, pl.ds(0, kv_cols)]), (wv_hbm, wkv.at[:, pl.ds(kv_cols, kv_cols)]),
                (wc_hbm, wc), (wu_hbm, wu), (wq_hbm, wq), (wb_hbm, wb),
            )
        )
    ]
    own_loads = [
        pltpu.make_async_copy(src, wo.at[sp, i], load_sem.at[6 + i]) for i, src in enumerate((woa_ref, woc_ref))
    ]
    barrier = pltpu.get_barrier_semaphore()

    def tell(sem, place):
        pl.semaphore_signal(sem, inc=1, device_id={"sp": place}, device_id_type=MESH)

    def tell_column(sem):
        guard(has_up)(lambda: tell(sem, up))
        guard(has_down)(lambda: tell(sem, down))

    column = has_up.astype(jnp.int32) + has_down.astype(jnp.int32)
    for place in (near, far):
        pl.semaphore_signal(barrier, inc=1, device_id={"tp": place}, device_id_type=MESH)
    tell(barrier, side)
    tell_column(barrier)
    for load in (*own_loads, *loads):
        load.start()
    pl.semaphore_wait(barrier, 3 + column)

    def push(src, dst, ssem, rsem, who):
        return pltpu.make_async_remote_copy(
            src_ref=src, dst_ref=dst, send_sem=ssem, recv_sem=rsem, device_id=who, device_id_type=MESH
        )

    to_far = [
        push(tok_ref.at[pl.ds(c * half, half)], xall.at[t, pl.ds(c * half, half)], tok_ssem.at[c], tok_rsem.at[c], {"tp": far})
        for c in range(2)
    ]
    to_near = push(tok_ref, xall.at[t], tok_ssem.at[2], tok_rsem.at[2], {"tp": near})
    relay = [
        push(xall.at[far, pl.ds(c * half, half)], xall.at[far, pl.ds(c * half, half)], tok_ssem.at[3 + c], tok_rsem.at[3 + c], {"tp": near})
        for c in range(2)
    ]
    for copy in to_far:
        copy.start()
    to_near.start()
    tell_column(near_by)

    early = t // 2

    def w_copy(h, c, d):
        view = wo.at[h, c // 2, pl.ds(pl.multiple_of((c % 2) * fpart, fpart), fpart)]
        return push(view, view, w_ssem.at[d, h, c], w_rsem.at[h, c], {"sp": ways[d]})

    def kv_copy(h, c, d):
        view = kv.at[h, early + (c - 4) * (1 - 2 * early)]
        return push(view, view, kv_ssem.at[d, h, c - 4], kv_rsem.at[h, c - 4], {"sp": ways[d]})

    def event(vals, arrive, leave):
        code = pick(vals)
        h, c = code // 128, code // 16 % 8
        for copy_of, low, high in ((w_copy, 0, 4), (kv_copy, 4, 6)):
            mine = [v for v in vals if v >= 0 and low <= v // 16 % 8 < high]
            if not mine:
                continue
            live = jnp.logical_and(code >= 16 * low, c < high) if low == 0 else c >= low
            live = jnp.logical_and(live, code >= 0)

            @pl.when(live)
            def _():
                if arrive and any(v % 2 for v in mine):
                    pl.when(code % 2 == 1)(lambda: copy_of(h, c, 0).wait_recv())
                for d in range(3):
                    if any(v // 2 // 2**d % 2 for v in mine):
                        pl.when(code // 2 // 2**d % 2 == 1)(lambda d=d: leave(copy_of(h, c, d)))

    def pump(point):
        for vals in EVENTS[point]:
            event(vals, True, lambda copy: copy.start())

    for load in own_loads:
        load.wait()
    pump(0)

    def dot(w):
        return jnp.dot(normed[...], w[...], preferred_element_type=F32)

    def project_kv(groups, pair):
        for i, g in enumerate(groups):
            x = (tok_ref[...] if g is None else xall[g]).astype(F32)
            inverse = lax.rsqrt(jnp.mean(x * x, axis=-1, keepdims=True) + 1e-06)
            at = rows * (t % 2 if i == 0 else 1 - t % 2)
            normed[pl.ds(pl.multiple_of(at, rows), rows)] = (x * inverse * gain_ref[...]).astype(BF16)
        both = dot(wkv).astype(BF16)
        kv[sp, pair, 0] = both[:, :kv_cols]
        kv[sp, pair, 1] = both[:, kv_cols:]

    def project_rest(pair, points):
        at = pl.ds(pl.multiple_of(pair * 2 * rows, 2 * rows), 2 * rows)
        gate = dot(wc).astype(BF16).astype(F32)
        pump(points[0])
        prod_sc[at] = (gate * dot(wu).astype(BF16).astype(F32)).astype(BF16)
        pump(points[1])
        q_sc[at] = dot(wq).astype(BF16)
        pump(points[2])
        gate_sc[at] = dot(wb).astype(BF16)
        pump(points[3])

    to_near.wait_recv()
    for load in loads[:2]:
        load.wait()
    project_kv((None, near), early)
    pump(1)
    for load in loads[2:]:
        load.wait()
    project_rest(early, (2, 3, 4, 5))
    pump(6)
    to_far[0].wait_recv()
    relay[0].start()
    pump(7)
    to_far[1].wait_recv()
    relay[1].start()
    for c in range(2):
        relay[c].wait_recv()
    project_kv((far, diag), 1 - early)
    pump(8)
    project_rest(1 - early, (9, 10, 11, 12))
    pl.semaphore_wait(near_by, column)
    halo = push(prod_sc.at[pl.ds(toks - HALO, HALO)], prev, halo_sem.at[0], halo_sem.at[1], {"sp": sp + 1})
    guard(sp < n - 1)(halo.start)

    key_i = lax.broadcasted_iota(jnp.int32, (toks, toks), 0)
    key_j = lax.broadcasted_iota(jnp.int32, (toks, toks), 1)
    later = (key_i > key_j).astype(F32).astype(BF16)
    scale = HEAD_DIM ** (-0.5)
    order = (t, far, near, diag)

    def visit(slot, masked):
        for h in range(heads):
            cols = pl.ds(h * HEAD_DIM, HEAD_DIM)
            kv_at = pl.ds((h // grouping) * HEAD_DIM, HEAD_DIM)
            keys = kv[slot, :, 0, :, kv_at].reshape(toks, HEAD_DIM)
            vals = kv[slot, :, 1, :, kv_at].reshape(toks, HEAD_DIM)
            s = lax.dot_general(q_sc[:, cols], keys, NT, preferred_element_type=F32) * scale + shift_ref[0, h]
            soft = softplus(s)
            if masked:
                soft = jnp.where(key_j < key_i, soft, 0.0)
            high = soft.astype(BF16)
            low = (soft - high.astype(F32)).astype(BF16)
            after = jnp.dot(high, later, preferred_element_type=F32) + jnp.dot(low, later, preferred_element_type=F32)
            weight = jnp.exp(s - soft - after)
            if masked:
                weight = jnp.where(key_j < key_i, weight, 0.0)
            part = jnp.dot(weight.astype(BF16), vals, preferred_element_type=F32)
            total = jnp.broadcast_to(after[:, 0:1] + soft[:, 0:1], (toks, HEAD_DIM))
            if masked:
                acc[:, cols] = part
                suffix[h] = total
            else:
                acc[:, cols] += jnp.exp(-suffix[h]) * part
                suffix[h] += total

    def convolve():
        @pl.when(sp == 0)
        def _():
            prev[...] = jnp.zeros(prev.shape, BF16)

        guard(sp > 0)(halo.wait_recv)
        ext[pl.ds(HALO, toks)] = prod_sc[...].astype(F32)
        ext[pl.ds(0, HALO)] = prev[...].astype(F32)
        summed = jnp.zeros((toks, ext.shape[1]), F32)
        for tap in range(CONV_K):
            summed = summed + taps_ref[tap : tap + 1, :] * ext[pl.ds(HALO - (CONV_K - 1) + tap, toks)]
        ext[pl.ds(HALO, toks)] = gate_sc[...].astype(F32) * summed
        for i, g in enumerate(order):
            acts[0, 1, pl.ds(i * rows, rows)] = ext[pl.ds(pl.multiple_of(HALO + g * rows, HALO), rows)].astype(BF16)

    def act_copy(i):
        return push(acts.at[0, i], acts.at[1, i], act_sem.at[0, i], act_sem.at[1, i], {"sp": host})

    visit(sp, True)
    pump(13)
    convolve()
    guard(outer)(lambda: act_copy(1).start())
    pump(14)
    for i in range(1, n):
        pump(14 + i)

        @pl.when(sp >= i)
        def _():
            visit(sp - i, False)

    for h in range(heads):
        spread = suffix[h].T[0:1, :]
        logw_ref[h : h + 1, :] = jnp.log(jnp.maximum(1.0 - jnp.exp(-spread), 0.05))
    for i, g in enumerate(order):
        acts[0, 0, pl.ds(i * rows, rows)] = acc[pl.ds(pl.multiple_of(g * rows, rows), rows)].astype(BF16)
    guard(outer)(lambda: act_copy(0).start())

    def d2d_copy(i):
        return push(snd.at[i], d2d.at[i], d2d_sem.at[0, i], d2d_sem.at[1, i], {"tp": near})

    def x_copy(i):
        return push(xsnd.at[i], xrcv.at[i], x_sem.at[0, i], x_sem.at[1, i], {"tp": far})

    def ret_copy(r):
        return push(gsnd.at[r], grcv.at[r], ret_sem.at[0, r], ret_sem.at[1, r], {"sp": host})

    def put(h, block):
        out_ref[:, pl.ds(pl.multiple_of(h * feats, feats), feats)] = block

    def active(i):
        vals = CELLS[i]
        if all(v >= 0 for v in vals):
            return lambda body: body()
        return pl.when(pick(vals) >= 0)

    def kinds(i, own, guest):
        code = pick(CELLS[i])
        if all(v < n for v in CELLS[i]):
            own(code)
        else:
            if any(0 <= v < n for v in CELLS[i]):
                pl.when(code < n)(lambda: own(code))
            pl.when(code >= n)(lambda: guest(code % n, code // n - 1))

    def first(i):
        @active(i)
        def _():
            def own(j):
                return None

            def visitor(j, r):
                @pl.when(r == 0)
                def _():
                    act_copy(1).wait_recv()
                    act_copy(0).wait_recv()

            kinds(i, own, visitor)
            code = pick(CELLS[i])
            j = code % n
            if all(v < n for v in CELLS[i]):
                a, b = acts.at[0, 0], acts.at[0, 1]
            else:
                who = jnp.minimum(code // n, 1)
                a, b = acts.at[who, 0], acts.at[who, 1]
            share = lax.dot_general(a[...], wo[j, 0], NT, preferred_element_type=F32)
            share = (share + lax.dot_general(b[...], wo[j, 1], NT, preferred_element_type=F32)).astype(BF16)
            snd[i] = share[2 * rows :]
            keep[i] = share[: 2 * rows]
            d2d_copy(i).start()

    def second(i):
        @active(i)
        def _():
            d2d_copy(i).wait_recv()
            xsnd[i] = (keep[i, pl.ds(rows, rows)].astype(F32) + d2d[i, pl.ds(rows, rows)].astype(F32)).astype(BF16)
            x_copy(i).start()

    def third(i):
        @active(i)
        def _():
            x_copy(i).wait_recv()
            own = keep[i, pl.ds(0, rows)].astype(F32) + d2d[i, pl.ds(0, rows)].astype(F32)
            done = (own + xrcv[i].astype(F32)).astype(BF16)

            def visitor(j, r):
                gsnd[r] = done
                ret_copy(r).start()

            kinds(i, lambda j: put(j, done), visitor)

    steps = len(CELLS)
    for i in range(steps):
        pump(22 + i)
        first(i)
        if i >= 1:
            second(i - 1)
        if i >= 3:
            third(i - 3)
    second(steps - 1)
    for i in range(steps - 3, steps):
        third(i)
    pump(22 + steps)
    for r in range(len(CELL_BACK)):
        @pl.when(pick(CELL_BACK[r]) >= 0)
        def _():
            ret_copy(r).wait_recv()
            put(pick(CELL_BACK[r]), grcv[r])

    for copy in (*to_far, to_near, *relay):
        copy.wait_send()
    guard(sp < n - 1)(halo.wait_send)
    for slots in EVENTS:
        for vals in slots:
            event(vals, False, lambda copy: copy.wait_send())

    @pl.when(outer)
    def _():
        for i in range(2):
            act_copy(i).wait_send()

    for i in range(steps):
        @active(i)
        def _():
            d2d_copy(i).wait_send()
            x_copy(i).wait_send()
            kinds(i, lambda j: None, lambda j, r: ret_copy(r).wait_send())


def grid_local(
    n, tokens, norm_gain, w_query, w_key, w_value, score_shift, w_conv_b, w_conv_c, w_conv_u,
    conv_kernel, w_out_att, w_out_conv,
):
    rows, d = tokens.shape
    toks = 4 * rows
    feats, att_cols = w_out_att.shape
    conv_cols = w_out_conv.shape[1]
    heads = score_shift.shape[0]
    kv_cols = w_key.shape[1]
    cells = len(CELLS)
    guests = len(CELL_BACK)
    vmem = pl.BlockSpec(memory_space=pltpu.VMEM)
    smem = pl.BlockSpec(memory_space=pltpu.SMEM)
    hbm = pl.BlockSpec(memory_space=pl.ANY)
    dma = pltpu.SemaphoreType.DMA
    regular = pltpu.SemaphoreType.REGULAR
    out, logw = pl.pallas_call(
        functools.partial(grid_kernel, n),
        out_shape=(
            jax.ShapeDtypeStruct((rows, n * feats), BF16),
            jax.ShapeDtypeStruct((heads, toks), F32),
        ),
        in_specs=[vmem, vmem, hbm, hbm, hbm, smem, hbm, hbm, hbm, vmem, hbm, hbm],
        out_specs=(vmem, vmem),
        scratch_shapes=[
            pltpu.VMEM(w_query.shape, BF16),
            pltpu.VMEM((d, 2 * kv_cols), BF16),
            *[pltpu.VMEM(w.shape, BF16) for w in (w_conv_b, w_conv_c, w_conv_u)],
            pltpu.VMEM((4, rows, d), BF16),
            pltpu.VMEM((2 * rows, d), BF16),
            pltpu.VMEM((toks, w_query.shape[1]), BF16),
            pltpu.VMEM((n, 2, 2, 2 * rows, kv_cols), BF16),
            pltpu.VMEM((n, 2, feats, att_cols), BF16),
            pltpu.VMEM((toks, conv_cols), BF16),
            pltpu.VMEM((toks, conv_cols), BF16),
            pltpu.VMEM((HALO, conv_cols), BF16),
            pltpu.VMEM((toks + HALO, conv_cols), F32),
            pltpu.VMEM((2, 2, toks, att_cols), BF16),
            pltpu.VMEM((toks, att_cols), F32),
            pltpu.VMEM((heads, toks, HEAD_DIM), F32),
            *[pltpu.VMEM((cells, 2 * rows, feats), BF16)] * 3,
            *[pltpu.VMEM((cells, rows, feats), BF16)] * 2,
            *[pltpu.VMEM((guests, rows, feats), BF16)] * 2,
            dma((8,)), dma((5,)), dma((5,)), dma((3, n, 2)), dma((n, 2)), dma((3, n, 4)), dma((n, 4)),
            dma((2,)), dma((2, cells)), dma((2, cells)), dma((2, 2)), dma((2, guests)), regular,
        ],
        compiler_params=pltpu.CompilerParams(
            collective_id=0, has_side_effects=True, vmem_limit_bytes=60 * 1024 * 1024
        ),
    )(
        tokens, norm_gain.reshape(1, d), w_query, w_key, w_value, score_shift.reshape(1, heads),
        w_conv_b, w_conv_c, w_conv_u, conv_kernel, w_out_att, w_out_conv,
    )
    return (out, logw.T)


def solution(mesh):
    n = mesh.shape["sp"]
    body = grid_local if n == len(CELLS[0]) and mesh.shape["tp"] == 4 else local
    return jax.shard_map(
        functools.partial(body, n),
        mesh=mesh,
        in_specs=(
            P(("sp", "tp"), None), P(), P(None, "tp"), P(None, "tp"), P(None, "tp"), P("tp"),
            P(None, "tp"), P(None, "tp"), P(None, "tp"), P(None, "tp"), P("sp", "tp"), P("sp", "tp"),
        ),
        out_specs=(P(("sp", "tp"), None), P("sp", "tp")),
        check_vma=False,
    )
```

```python
import functools

import jax
import jax.numpy as jnp
from jax import lax
from jax.experimental import pallas as pl
from jax.experimental.pallas import tpu as pltpu
from jax.sharding import PartitionSpec as P

HEAD_DIM = 128
CONV_K = 3
HALO = 16
F32 = jnp.float32
BF16 = jnp.bfloat16
MESH = pl.DeviceIdType.MESH
NT = (((1,), (1,)), ((), ()))
EVENTS = [[(8, 18), (136, 146), (266, 276), (398,), (518, 536), (648, 662), (780,), (908,)],
 [(74, 24, 34),
  (194, 152, 162),
  (330, 274, 292, 312),
  (450, 410, 420),
  (586, 530, 548, 568),
  (706, 686),
  (840, 792, 820),
  (920, 932)],
 [(), (), (), (), (), (), (), ()],
 [(), (), (), (), (), (), (), ()],
 [(), (184,), (308,), (436,), (), (692,), (), (956,)],
 [(), (), (), (), (), (), (), ()],
 [(40, 50),
  (178,),
  (290, 521, 75, 389),
  (418, 203, 261),
  (546, 265, 645, 331),
  (690, 905, 459, 533),
  (808, 585),
  (713, 773)],
 [(90, 56, 131), (210, 3, 425), (346,), (466,), (602, 821), (722, 937), (856, 917), (665,)],
 [(297,),
  (441,),
  (405, 306, 553, 645),
  (661, 434, 169, 697, 677),
  (562, 281),
  (900, 387, 409, 932),
  (521,),
  (789, 681)],
 [(106, 419),
  (226, 35, 265),
  (91, 362),
  (219, 482),
  (75, 347, 618, 917),
  (203, 475, 738),
  (329, 601, 872),
  (457, 729, 805)],
 [(), (), (), (), (), (), (), ()],
 [(), (), (825,), (185,), (), (), (661,), ()],
 [(), (), (), (), (), (), (), ()],
 [(313,), (), (165,), (517,), (933,), (565,), (), ()],
 [(), (665,), (), (), (920,), (793,), (537,), (697,)],
 [(), (), (), (), (), (), (), ()],
 [(),
  (291, 681, 65, 81, 97),
  (107, 19, 137, 693, 35, 917, 51, 193, 209, 225),
  (235, 147, 533, 321, 337, 353),
  (91, 363, 107, 642, 661, 313, 291, 789, 25, 449, 465, 481),
  (219, 949, 491, 235, 259, 577, 593, 609),
  (73, 345, 617, 89, 361, 105, 693, 553, 705, 721, 737),
  (517, 201, 473, 745, 833, 849, 865)],
 [(), (), (), (178, 9), (930,), (), (), (217,)],
 [(),
  (),
  (),
  (901, 2, 569, 65, 81, 97),
  (193, 209, 225),
  (419, 773, 809, 277, 153, 321, 337, 353),
  (569, 449, 465, 481),
  (489, 233, 393, 577, 593, 609)],
 [(), (), (), (), (), (274,), (), ()],
 [(), (), (), (), (), (65, 81, 97), (193, 209, 225), (265, 321, 337, 353)],
 [(), (), (), (), (), (), (649,), ()],
 [(), (), (), (), (), (), (), (65, 81, 97)],
 [(), (), (162, 933), (), (403, 41, 805), (435, 804, 185), (), (425,)],
 [(385, 401, 433), (17, 49), (1,), (549,), (), (), (), (281, 529, 545, 561)],
 [(408, 257, 273),
  (521, 537, 385, 401),
  (130, 793, 565, 417, 433),
  (546, 953, 129),
  (306, 57, 673, 689),
  (913,),
  (297, 389, 673),
  (441, 641)],
 [(649, 434, 145, 161, 177),
  (905, 643, 553, 689),
  (434, 949, 657, 673),
  (933, 819, 777, 948, 130, 273, 289, 305),
  (149, 769),
  (916, 307, 9, 513, 545),
  (897, 929, 945),
  (289, 305)],
 [(697, 675, 657),
  (913, 929, 945),
  (946, 769, 801),
  (641,),
  (169, 129, 177),
  (21, 819),
  (409, 421, 257, 273, 305),
  (817,)],
 [(921, 531, 569, 899, 929, 945), (561,), (), (276, 290, 785, 801), (1,), (53, 33), (433,), (401,)],
 [(513, 545), (273, 305), (529,), (), (), (), (), ()],
 [(), (), (145, 177), (913,), (), (129, 161), (), ()],
 [(), (), (897,), (17, 33, 49), (897, 945), (), (), ()],
 [(), (), (), (), (385, 417, 433), (289,), (), ()],
 [(), (), (), (), (), (), (), ()]]
CELLS = [(0, 1, 2, 3, 4, 5, 6, 7),
 (3, 0, 0, 4, 2, 3, 4, 4),
 (2, 3, 3, 1, 5, 7, 5, 5),
 (1, 5, 5, 2, 6, 4, 7, 2),
 (5, 7, 14, 5, 1, 6, 2, 6),
 (7, 4, 6, 14, 0, 8, 3, 3),
 (4, 2, 4, 6, 8, 0, -1, -1),
 (-1, -1, 1, 7, 17, 17, -1, -1),
 (-1, -1, 7, 0, 7, 1, -1, -1),
 (-1, -1, -1, -1, 3, 2, -1, -1)]
CELL_BACK = [(6, 6, -1, -1, -1, -1, 0, 0), (-1, -1, -1, -1, -1, -1, 1, 1)]


def softplus(z):
    u = jnp.exp(-jnp.abs(z))
    small = u * (1.0 - u * (0.5 - u * (1.0 / 3.0 - u * 0.25)))
    return jnp.maximum(z, 0.0) + jnp.where(u < 0.01, small, jnp.log(1.0 + u))


def kernel(
    n,
    tok_ref, gain_ref, wq_hbm, wk_hbm, wv_hbm, shift_ref, wb_hbm, wc_hbm, wu_hbm, taps_ref, woa_ref, woc_ref,
    out_ref, logw_ref,
    wq, wk, wv, wb, wc, wu, xall, normed, q_sc, kv, wo, gate_sc, prod_sc, prev, ext, attn, conv, partial, totals,
    snd, keep, d2d, xsnd, xrcv,
    load_sem, tok_ssem, tok_rsem, kv_sem, w_sem, halo_sem, d2d_sem, x_sem,
):
    sp = lax.axis_index("sp")
    t = lax.axis_index("tp")
    near = t + 1 - 2 * (t % 2)
    far = t + 2 - 4 * ((t // 2) % 2)
    diag = near + 2 - 4 * ((near // 2) % 2)
    pos = jnp.where(sp % 2 == 0, sp // 2, n - 1 - sp // 2)

    def ring(place):
        place = (place + 2 * n) % n
        return jnp.where(place < n // 2, 2 * place, 2 * (n - 1 - place) + 1)

    right, left = ring(pos + 1), ring(pos - 1)
    following, leading = (sp + 1) % n, (sp + n - 1) % n
    rows = tok_ref.shape[0]
    toks = 4 * rows
    half = rows // 2
    fpart = wo.shape[2] // 2
    heads = q_sc.shape[1] // HEAD_DIM
    kv_cols = kv.shape[4]
    grouping = heads // (kv_cols // HEAD_DIM)

    loads = [
        pltpu.make_async_copy(src, dst, load_sem.at[i])
        for i, (src, dst) in enumerate(
            ((wk_hbm, wk), (wv_hbm, wv), (wq_hbm, wq), (wc_hbm, wc), (wu_hbm, wu), (wb_hbm, wb))
        )
    ]
    own_loads = [
        pltpu.make_async_copy(src, wo.at[sp, i], load_sem.at[6 + i]) for i, src in enumerate((woa_ref, woc_ref))
    ]
    barrier = pltpu.get_barrier_semaphore()
    for place in (right, left, following, leading):
        pl.semaphore_signal(barrier, inc=1, device_id={"sp": place}, device_id_type=MESH)
    for place in (near, far):
        pl.semaphore_signal(barrier, inc=1, device_id={"tp": place}, device_id_type=MESH)
    for load in (*own_loads, *loads):
        load.start()
    pl.semaphore_wait(barrier, 6)

    def push(src, dst, ssem, rsem, who):
        return pltpu.make_async_remote_copy(
            src_ref=src, dst_ref=dst, send_sem=ssem, recv_sem=rsem, device_id=who, device_id_type=MESH
        )

    to_far = [
        push(tok_ref.at[pl.ds(c * half, half)], xall.at[t, pl.ds(c * half, half)], tok_ssem.at[c], tok_rsem.at[c], {"tp": far})
        for c in range(2)
    ]
    to_near = push(tok_ref, xall.at[t], tok_ssem.at[2], tok_rsem.at[2], {"tp": near})
    relay = [
        push(xall.at[far, pl.ds(c * half, half)], xall.at[far, pl.ds(c * half, half)], tok_ssem.at[3 + c], tok_rsem.at[3 + c], {"tp": near})
        for c in range(2)
    ]
    for copy in to_far:
        copy.start()
    to_near.start()

    last = n // 2

    def hop(part, sem, way, step, chunk):
        block = ring(pos - (step - 1)) if way == 0 else ring(pos + (step - 1))
        view = part(block, chunk, step)
        return push(
            view[0], view[1], sem.at[0, way, step - 1, chunk], sem.at[1, way, step - 1, chunk],
            {"sp": right if way == 0 else left},
        )

    def ways(step, chunk, chunks):
        if isinstance(step, int) and step == last:
            return (0,) if chunk < chunks // 2 else (1,)
        return (0, 1)

    early = t // 2

    def kv_part(block, chunk, step):
        view = kv.at[block, early + chunk * (1 - 2 * early)]
        return view, view

    def w_part(block, chunk, step):
        view = wo.at[block, chunk // 2, pl.ds(pl.multiple_of((chunk % 2) * fpart, fpart), fpart)]
        return view, view

    rings = {"kv": (kv_part, kv_sem, 2), "w": (w_part, w_sem, 4)}

    def emit(name, step, chunk):
        part, sem, chunks = rings[name]
        for way in ways(step, chunk, chunks):
            hop(part, sem, way, step, chunk).start()

    def take(name, step, chunk, onward=None):
        part, sem, chunks = rings[name]
        for way in ways(step, chunk, chunks):
            hop(part, sem, way, step, chunk).wait_recv()
        if onward or (onward is None and step < last):
            emit(name, step + 1, chunk)

    for load in own_loads:
        load.wait()
    for chunk in (0, 1):
        emit("w", 1, chunk)

    def dot(w):
        return jnp.dot(normed[...], w[...], preferred_element_type=F32).astype(BF16)

    def project_kv(groups, pair):
        for i, g in enumerate(groups):
            x = (tok_ref[...] if g is None else xall[g]).astype(F32)
            inverse = lax.rsqrt(jnp.mean(x * x, axis=-1, keepdims=True) + 1e-06)
            at = rows * (t % 2 if i == 0 else 1 - t % 2)
            normed[pl.ds(pl.multiple_of(at, rows), rows)] = (x * inverse * gain_ref[...]).astype(BF16)
        kv[sp, pair, 0] = dot(wk)
        kv[sp, pair, 1] = dot(wv)

    def project_rest(pair):
        at = pl.ds(pl.multiple_of(pair * 2 * rows, 2 * rows), 2 * rows)
        prod_sc[at] = (dot(wc).astype(F32) * dot(wu).astype(F32)).astype(BF16)
        q_sc[at] = dot(wq)
        gate_sc[at] = dot(wb)

    to_near.wait_recv()
    for load in loads[:2]:
        load.wait()
    project_kv((None, near), early)
    emit("kv", 1, 0)
    for chunk in (2, 3):
        emit("w", 1, chunk)
    for load in loads[2:]:
        load.wait()
    project_rest(early)
    to_far[0].wait_recv()
    relay[0].start()
    take("kv", 1, 0)
    take("w", 1, 0)
    to_far[1].wait_recv()
    relay[1].start()
    for c in range(2):
        relay[c].wait_recv()
    project_kv((far, diag), 1 - early)
    emit("kv", 1, 1)
    take("w", 1, 1)
    take("w", 1, 2)
    project_rest(1 - early)
    halo = push(prod_sc.at[pl.ds(toks - HALO, HALO)], prev, halo_sem.at[0], halo_sem.at[1], {"sp": following})
    halo.start()

    key_i = lax.broadcasted_iota(jnp.int32, (toks, toks), 0)
    key_j = lax.broadcasted_iota(jnp.int32, (toks, toks), 1)
    later = (key_i > key_j).astype(F32).astype(BF16)
    lane = lax.broadcasted_iota(jnp.int32, (toks, totals.shape[2]), 1)
    scale = HEAD_DIM ** (-0.5)
    order = (t, far, near, diag)

    def visit(slot, masked):
        for h in range(heads):
            cols = pl.ds(h * HEAD_DIM, HEAD_DIM)
            kv_at = pl.ds((h // grouping) * HEAD_DIM, HEAD_DIM)
            keys = kv[slot, :, 0, :, kv_at].reshape(toks, HEAD_DIM)
            vals = kv[slot, :, 1, :, kv_at].reshape(toks, HEAD_DIM)
            z = lax.dot_general(q_sc[:, cols], keys, NT, preferred_element_type=F32) * scale + shift_ref[0, h]
            soft = softplus(z)
            if masked:
                soft = jnp.where(key_j < key_i, soft, 0.0)
            high = soft.astype(BF16)
            low = (soft - high.astype(F32)).astype(BF16)
            after = jnp.dot(high, later, preferred_element_type=F32) + jnp.dot(low, later, preferred_element_type=F32)
            weight = jnp.exp(z - soft - after)
            if masked:
                weight = jnp.where(key_j < key_i, weight, 0.0)
            partial[slot, :, cols] = jnp.dot(weight.astype(BF16), vals, preferred_element_type=F32)
            total = after[:, 0:1] + soft[:, 0:1]
            totals[h] = jnp.where(lane == slot, total, totals[h])

    def visit_at(step, both=True):
        def side(i, carry):
            slot = ring(pos + (2 * i - 1) * step)

            @pl.when(slot < sp)
            def _():
                visit(slot, False)

            return carry

        lax.fori_loop(0, 2 if both else 1, side, 0)

    totals[...] = jnp.zeros(totals.shape, F32)
    visit(sp, True)

    def w_event(m):
        return m // 4 + 1, m % 4

    def body(s, carry):
        if n > 4:
            take("kv", s + 1, 0, True)
            take("kv", s, 1, True)
            take("w", *w_event(2 * s + 1), True)
            take("w", *w_event(2 * s + 2), True)
            visit_at(s)
        return carry

    def convolve():
        halo.wait_recv()
        ext[pl.ds(HALO, toks)] = prod_sc[...].astype(F32)
        ext[pl.ds(0, HALO)] = jnp.where(sp == 0, 0.0, prev[...].astype(F32))
        summed = jnp.zeros((toks, ext.shape[1]), F32)
        for tap in range(CONV_K):
            summed = summed + taps_ref[tap : tap + 1, :] * ext[pl.ds(HALO - (CONV_K - 1) + tap, toks)]
        ext[pl.ds(HALO, toks)] = gate_sc[...].astype(F32) * summed
        for i, g in enumerate(order):
            conv[pl.ds(i * rows, rows)] = ext[pl.ds(pl.multiple_of(HALO + g * rows, HALO), rows)].astype(BF16)

    loops = max(last - 3, 0)
    lax.fori_loop(1, 1 + loops, body, 0)
    w_done = 3 + 2 * loops
    convolve()
    for s in range(1 + loops, last + 1):
        if s + 1 <= last:
            take("kv", s + 1, 0)
        take("kv", s, 1)
        for m in range(w_done, w_done + 2 if s < last else w_done + 1):
            take("w", *w_event(m))
            w_done += 1
        visit_at(s, s < last)

    def combine(i, carry):
        slot = sp - i
        suffixes = []
        for h in range(heads):
            cols = pl.ds(h * HEAD_DIM, HEAD_DIM)
            suffix = carry[h]
            ext[pl.ds(HALO, toks), cols] += jnp.exp(-suffix) * partial[slot, :, cols]
            total = jnp.sum(jnp.where(lane == slot, totals[h], 0.0), axis=1, keepdims=True)
            suffixes.append(suffix + total)
        return tuple(suffixes)

    ext[...] = jnp.zeros(ext.shape, F32)
    suffixes = lax.fori_loop(0, sp + 1, combine, tuple(jnp.zeros((toks, 1), F32) for _ in range(heads)))
    for h in range(heads):
        spread = jnp.broadcast_to(suffixes[h], (toks, 128)).T[0:1, :]
        logw_ref[h : h + 1, :] = jnp.log(jnp.maximum(1.0 - jnp.exp(-spread), 0.05))
    for i, g in enumerate(order):
        attn[pl.ds(i * rows, rows)] = ext[pl.ds(pl.multiple_of(HALO + g * rows, HALO), rows), 0 : attn.shape[1]].astype(BF16)

    def block_of(i):
        return ring(pos - (i + 1) // 2) if i % 2 else ring(pos + i // 2)

    def d2d_copy(i):
        return push(snd.at[i], d2d.at[i], d2d_sem.at[0, i], d2d_sem.at[1, i], {"tp": near})

    def x_copy(i):
        return push(xsnd.at[i], xrcv.at[i], x_sem.at[0, i], x_sem.at[1, i], {"tp": far})

    def first(i):
        j = block_of(i)
        share = lax.dot_general(attn[...], wo[j, 0], NT, preferred_element_type=F32)
        share = (share + lax.dot_general(conv[...], wo[j, 1], NT, preferred_element_type=F32)).astype(BF16)
        snd[i] = share[2 * rows :]
        keep[i] = share[: 2 * rows]
        d2d_copy(i).start()

    def second(i):
        d2d_copy(i).wait_recv()
        xsnd[i] = (keep[i, pl.ds(rows, rows)].astype(F32) + d2d[i, pl.ds(rows, rows)].astype(F32)).astype(BF16)
        x_copy(i).start()

    def third(i):
        x_copy(i).wait_recv()
        own = keep[i, pl.ds(0, rows)].astype(F32) + d2d[i, pl.ds(0, rows)].astype(F32)
        done = (own + xrcv[i].astype(F32)).astype(BF16)
        if len(out_ref.shape) == 3:
            out_ref[block_of(i)] = done
        else:
            feats = keep.shape[2]
            out_ref[:, pl.ds(pl.multiple_of(block_of(i) * feats, feats), feats)] = done

    for i in range(n):
        while w_done < max(4 * ((i + 1) // 2), min(10 + i, 4 * last)):
            take("w", *w_event(w_done))
            w_done += 1
        first(i)
        if i >= 1:
            second(i - 1)
        if i >= 3:
            third(i - 3)
    second(n - 1)
    for i in range(max(n - 3, 0), n):
        third(i)

    for copy in (*to_far, to_near, *relay, halo):
        copy.wait_send()
    for part, sem, chunks in rings.values():
        for step in range(1, last + 1):
            for chunk in range(chunks):
                for way in ways(step, chunk, chunks):
                    hop(part, sem, way, step, chunk).wait_send()
    for i in range(n):
        d2d_copy(i).wait_send()
        x_copy(i).wait_send()


def local(
    n, tokens, norm_gain, w_query, w_key, w_value, score_shift, w_conv_b, w_conv_c, w_conv_u,
    conv_kernel, w_out_att, w_out_conv,
):
    rows, d = tokens.shape
    toks = 4 * rows
    feats, att_cols = w_out_att.shape
    conv_cols = w_out_conv.shape[1]
    heads = score_shift.shape[0]
    kv_cols = w_key.shape[1]
    vmem = pl.BlockSpec(memory_space=pltpu.VMEM)
    smem = pl.BlockSpec(memory_space=pltpu.SMEM)
    hbm = pl.BlockSpec(memory_space=pl.ANY)
    dma = pltpu.SemaphoreType.DMA
    wide = feats % 128 == 0
    out, logw = pl.pallas_call(
        functools.partial(kernel, n),
        out_shape=(
            jax.ShapeDtypeStruct((rows, n * feats) if wide else (n, rows, feats), BF16),
            jax.ShapeDtypeStruct((heads, toks), F32),
        ),
        in_specs=[vmem, vmem, hbm, hbm, hbm, smem, hbm, hbm, hbm, vmem, hbm, hbm],
        out_specs=(vmem, vmem),
        scratch_shapes=[
            *[pltpu.VMEM(w.shape, BF16) for w in (w_query, w_key, w_value, w_conv_b, w_conv_c, w_conv_u)],
            pltpu.VMEM((4, rows, d), BF16),
            pltpu.VMEM((2 * rows, d), BF16),
            pltpu.VMEM((toks, w_query.shape[1]), BF16),
            pltpu.VMEM((n, 2, 2, 2 * rows, kv_cols), BF16),
            pltpu.VMEM((n, 2, feats, att_cols), BF16),
            pltpu.VMEM((toks, conv_cols), BF16),
            pltpu.VMEM((toks, conv_cols), BF16),
            pltpu.VMEM((HALO, conv_cols), BF16),
            pltpu.VMEM((toks + HALO, max(conv_cols, att_cols)), F32),
            pltpu.VMEM((toks, att_cols), BF16),
            pltpu.VMEM((toks, conv_cols), BF16),
            pltpu.VMEM((n, toks, att_cols), F32),
            pltpu.VMEM((heads, toks, 128), F32),
            pltpu.VMEM((n, 2 * rows, feats), BF16),
            pltpu.VMEM((n, 2 * rows, feats), BF16),
            pltpu.VMEM((n, 2 * rows, feats), BF16),
            pltpu.VMEM((n, rows, feats), BF16),
            pltpu.VMEM((n, rows, feats), BF16),
            dma((8,)), dma((5,)), dma((5,)), dma((2, 2, n // 2, 2)), dma((2, 2, n // 2, 4)), dma((2,)), dma((2, n)), dma((2, n)),
        ],
        compiler_params=pltpu.CompilerParams(
            collective_id=0, has_side_effects=True, vmem_limit_bytes=60 * 1024 * 1024
        ),
    )(
        tokens, norm_gain.reshape(1, d), w_query, w_key, w_value, score_shift.reshape(1, heads),
        w_conv_b, w_conv_c, w_conv_u, conv_kernel, w_out_att, w_out_conv,
    )
    if not wide:
        out = out.transpose(1, 0, 2).reshape(rows, n * feats)
    return (out, logw.T)

def soft_plus(z):
    u = jnp.exp(-jnp.abs(z))
    small = u - (u * u) * (0.5 - u * (1.0 / 3.0))
    return jnp.maximum(z, 0.0) + jnp.where(u < 0.005, small, jnp.log(1.0 + u))


def grid_kernel(
    n,
    tok_hbm, gain_hbm, wq_hbm, wk_hbm, wv_hbm, shift_hbm, wb_hbm, wc_hbm, wu_hbm, taps_hbm, woa_ref, woc_ref,
    out_ref, logw_ref,
    gain_ref, shift_ref, taps_ref, wq, wkv, wb, wc, wu, xall, normed, q_sc, kv, wo, gate_sc, prod_sc, prev, ext, acts, acc, suffix,
    snd, keep, d2d, xsnd, xrcv, gsnd, grcv,
    load_sem, tok_ssem, tok_rsem, kv_ssem, kv_rsem, w_ssem, w_rsem, halo_sem, d2d_sem, x_sem,
    act_sem, ret_sem, near_by,
):
    sp = lax.axis_index("sp")
    t = lax.axis_index("tp")
    z = sp // 2
    y = sp % 2
    near = t + 1 - 2 * (t % 2)
    far = t + 2 - 4 * ((t // 2) % 2)
    diag = near + 2 - 4 * ((near // 2) % 2)
    up, down, side = sp + 2, sp - 2, sp + 1 - 2 * y
    ways = (up, down, side)
    host = sp + 2 - 4 * (z % 2)
    levels = n // 2
    has_up, has_down = z < levels - 1, z > 0
    outer = jnp.logical_or(z == 0, z == levels - 1)
    rows = tok_hbm.shape[0]
    toks = 4 * rows
    half = rows // 2
    fpart = wo.shape[2] // 2
    feats = wo.shape[2]
    heads = q_sc.shape[0] // toks
    kv_cols = kv.shape[4]
    grouping = heads // (kv_cols // HEAD_DIM)

    def pick(vals):
        out = vals[0]
        for i in range(1, n):
            if vals[i] != vals[0] or not isinstance(out, int):
                out = jnp.where(sp == i, vals[i], out)
        return out

    def guard(cond):
        return pl.when(cond)

    loads = [
        pltpu.make_async_copy(src, dst, load_sem.at[i])
        for i, (src, dst) in enumerate(
            (
                (wk_hbm, wkv.at[:, pl.ds(0, kv_cols)]), (wv_hbm, wkv.at[:, pl.ds(kv_cols, kv_cols)]),
                (wc_hbm, wc), (wu_hbm, wu), (wq_hbm, wq), (wb_hbm, wb),
            )
        )
    ]
    own_loads = [
        pltpu.make_async_copy(src, wo.at[sp, i], load_sem.at[6 + i]) for i, src in enumerate((woa_ref, woc_ref))
    ]
    tok_loads = [
        pltpu.make_async_copy(tok_hbm.at[pl.ds(c * half, half)], xall.at[t, pl.ds(c * half, half)], load_sem.at[8 + c])
        for c in range(2)
    ]
    small_loads = [
        pltpu.make_async_copy(src, dst, load_sem.at[10 + i])
        for i, (src, dst) in enumerate(((gain_hbm, gain_ref), (shift_hbm, shift_ref), (taps_hbm, taps_ref)))
    ]
    barrier = pltpu.get_barrier_semaphore()

    def tell(sem, place):
        pl.semaphore_signal(sem, inc=1, device_id={"sp": place}, device_id_type=MESH)

    def tell_column(sem):
        guard(has_up)(lambda: tell(sem, up))
        guard(has_down)(lambda: tell(sem, down))

    column = has_up.astype(jnp.int32) + has_down.astype(jnp.int32)
    for place in (near, far):
        pl.semaphore_signal(barrier, inc=1, device_id={"tp": place}, device_id_type=MESH)
    tell(barrier, side)
    tell_column(barrier)
    for load in (*tok_loads, *own_loads, *small_loads, *loads):
        load.start()
    pl.semaphore_wait(barrier, 3 + column)

    def push(src, dst, ssem, rsem, who):
        return pltpu.make_async_remote_copy(
            src_ref=src, dst_ref=dst, send_sem=ssem, recv_sem=rsem, device_id=who, device_id_type=MESH
        )

    to_far = [
        push(xall.at[t, pl.ds(c * half, half)], xall.at[t, pl.ds(c * half, half)], tok_ssem.at[c], tok_rsem.at[c], {"tp": far})
        for c in range(2)
    ]
    to_near = push(xall.at[t], xall.at[t], tok_ssem.at[2], tok_rsem.at[2], {"tp": near})
    relay = [
        push(xall.at[far, pl.ds(c * half, half)], xall.at[far, pl.ds(c * half, half)], tok_ssem.at[3 + c], tok_rsem.at[3 + c], {"tp": near})
        for c in range(2)
    ]
    for load, copy in zip(tok_loads, to_far):
        load.wait()
        copy.start()
    to_near.start()
    tell_column(near_by)

    early = t // 2

    def hop_copy(site, h, c, d):
        if c < 4:
            view = wo.at[h, c // 2, pl.ds(c % 2 * fpart, fpart)]
            sems = (w_ssem.at[d, h, c], w_rsem.at[h, c])
        else:
            view = kv.at[h, early] if c == 4 else kv.at[h, 1 - early, :, pl.ds((c - 5) * rows, rows)]
            sems = (kv_ssem.at[d, h, c - 4], kv_rsem.at[h, c - 4])
        return push(view, view, *sems, {"sp": (site + 2, site - 2, site ^ 1)[d]})

    def at_site(bodies, low=0, high=n):
        if all(body is None for body in bodies[low:high]):
            return
        if high - low == 1:
            bodies[low]()
            return
        mid = (low + high) // 2
        lax.cond(sp < mid, lambda: at_site(bodies, low, mid), lambda: at_site(bodies, mid, high))

    def events(point, arrive, leave):
        def body_of(site, codes):
            def body():
                for code in codes:
                    h, c = code // 128, code // 16 % 8
                    if arrive and code % 2:
                        hop_copy(site, h, c, 2).wait_recv()
                    for d in range(3):
                        if code // 2 // 2**d % 2:
                            leave(hop_copy(site, h, c, d))

            return body if codes else None

        at_site([body_of(site, codes) for site, codes in enumerate(EVENTS[point])])

    def pump(point):
        events(point, True, lambda copy: copy.start())

    for load in own_loads:
        load.wait()
    pump(0)
    for load in small_loads:
        load.wait()

    def dot(w):
        return jnp.dot(normed[...], w[...], preferred_element_type=F32)

    def normalize(g, same, low, count):
        x = xall[g, pl.ds(low, count)].astype(F32)
        inverse = lax.rsqrt(jnp.mean(x * x, axis=-1, keepdims=True) + 1e-06)
        at = rows * (t % 2 if same else 1 - t % 2) + low
        normed[pl.ds(pl.multiple_of(at, half), count)] = (x * inverse * gain_ref[...]).astype(BF16)

    def project_early():
        normalize(t, True, 0, rows)
        normalize(near, False, 0, rows)
        both = dot(wkv).astype(BF16)
        kv[sp, early, 0] = both[:, :kv_cols]
        kv[sp, early, 1] = both[:, kv_cols:]

    def project_late(c):
        normalize(far, True, c * half, half)
        normalize(diag, False, c * half, half)
        some = jnp.concatenate([normed[pl.ds(c * half, half)], normed[pl.ds(rows + c * half, half)]], axis=0)
        both = jnp.dot(some, wkv[...], preferred_element_type=F32).astype(BF16)
        at = pl.ds(c * rows, rows)
        kv[sp, 1 - early, 0, at] = both[:, :kv_cols]
        kv[sp, 1 - early, 1, at] = both[:, kv_cols:]

    def project_rest(pair, points):
        at = pl.ds(pl.multiple_of(pair * 2 * rows, 2 * rows), 2 * rows)
        gate = dot(wc).astype(BF16).astype(F32)
        pump(points[0])
        prod_sc[at] = (gate * dot(wu).astype(BF16).astype(F32)).astype(BF16)
        pump(points[1])
        queries = dot(wq).astype(BF16)
        for h in range(heads):
            to = pl.ds(pl.multiple_of(h * toks + pair * 2 * rows, 2 * rows), 2 * rows)
            q_sc[to] = queries[:, h * HEAD_DIM : (h + 1) * HEAD_DIM]
        pump(points[2])
        gate_sc[at] = dot(wb).astype(BF16)
        pump(points[3])

    to_near.wait_recv()
    for load in loads[:2]:
        load.wait()
    project_early()
    pump(1)
    for load in loads[2:]:
        load.wait()
    project_rest(early, (2, 3, 4, 5))
    for c in range(2):
        pump(6 + 2 * c)
        to_far[c].wait_recv()
        relay[c].start()
        relay[c].wait_recv()
        project_late(c)
        pump(7 + 2 * c)
    project_rest(1 - early, (10, 11, 12, 13))
    pl.semaphore_wait(near_by, column)
    halo = push(prod_sc.at[pl.ds(toks - HALO, HALO)], prev, halo_sem.at[0], halo_sem.at[1], {"sp": sp + 1})
    guard(sp < n - 1)(halo.start)

    def spot(index):
        index = index % toks
        pair, sub = index // (2 * rows), index % (2 * rows)
        moved = sub % rows // half * rows + sub // rows * half + sub % half
        return jnp.where(pair == early, index, pair * 2 * rows + moved)

    later = spot(lax.broadcasted_iota(jnp.int32, (2 * toks, 1), 0)) > spot(lax.broadcasted_iota(jnp.int32, (1, toks), 1))
    later = later.astype(F32).astype(BF16)
    stacked = grouping * toks
    query = lax.broadcasted_iota(jnp.int32, (stacked, 1), 0) % toks
    causal = spot(lax.broadcasted_iota(jnp.int32, (1, toks), 1)) < query
    head_of = lax.broadcasted_iota(jnp.int32, (stacked, 1), 0) // toks
    scale = HEAD_DIM ** (-0.5)
    order = (t, far, near, diag)

    def visit(slot, masked):
        for g in range(heads // grouping):
            at = pl.ds(g * stacked, stacked)
            kv_at = pl.ds(g * HEAD_DIM, HEAD_DIM)
            keys = kv[slot, :, 0, :, kv_at].reshape(toks, HEAD_DIM)
            vals = kv[slot, :, 1, :, kv_at].reshape(toks, HEAD_DIM)
            shift = shift_ref[0:1, g * grouping : g * grouping + 1]
            for h in range(1, grouping):
                shift = jnp.where(head_of < h, shift, shift_ref[0:1, g * grouping + h : g * grouping + h + 1])
            s = lax.dot_general(q_sc[at], keys, NT, preferred_element_type=F32) * scale + shift
            soft = soft_plus(s)
            if masked:
                soft = jnp.where(causal, soft, 0.0)
            high = soft.astype(BF16)
            low = (soft - high.astype(F32)).astype(BF16)
            after = jnp.dot(jnp.concatenate([high, low], axis=1), later, preferred_element_type=F32)
            weight = jnp.exp(s - soft - after)
            if masked:
                weight = jnp.where(causal, weight, 0.0)
            part = jnp.dot(weight.astype(BF16), vals, preferred_element_type=F32)
            total = jnp.broadcast_to(after[:, 0:1] + soft[:, 0:1], (stacked, HEAD_DIM))
            if masked:
                acc[at] = part
                suffix[at] = total
            else:
                acc[at] += jnp.exp(-suffix[at]) * part
                suffix[at] += total

    def convolve():
        @pl.when(sp == 0)
        def _():
            prev[...] = jnp.zeros(prev.shape, BF16)

        guard(sp > 0)(halo.wait_recv)
        ext[pl.ds(HALO, toks)] = prod_sc[...].astype(F32)
        ext[pl.ds(0, HALO)] = prev[...].astype(F32)
        summed = jnp.zeros((toks, ext.shape[1]), F32)
        for tap in range(CONV_K):
            summed = summed + taps_ref[tap : tap + 1, :] * ext[pl.ds(HALO - (CONV_K - 1) + tap, toks)]
        ext[pl.ds(HALO, toks)] = gate_sc[...].astype(F32) * summed
        for i, g in enumerate(order):
            acts[0, 1, pl.ds(i * rows, rows)] = ext[pl.ds(pl.multiple_of(HALO + g * rows, HALO), rows)].astype(BF16)

    def act_copy(i):
        return push(acts.at[0, i], acts.at[1, i], act_sem.at[0, i], act_sem.at[1, i], {"sp": host})

    visit(sp, True)
    pump(14)
    convolve()
    guard(outer)(lambda: act_copy(1).start())
    pump(15)
    for i in range(1, n):
        pump(15 + i)

        @pl.when(sp >= i)
        def _():
            visit(sp - i, False)

    for h in range(heads):
        for i, g in enumerate(order):
            have = acc[pl.ds(pl.multiple_of(h * toks + g * rows, rows), rows)]
            acts[0, 0, pl.ds(i * rows, rows), pl.ds(h * HEAD_DIM, HEAD_DIM)] = have.astype(BF16)
    guard(outer)(lambda: act_copy(0).start())
    for h in range(heads):
        spread = suffix[pl.ds(h * toks, toks)].T[0:1, :]
        logw_ref[h : h + 1, :] = jnp.log(jnp.maximum(1.0 - jnp.exp(-spread), 0.05))

    def d2d_copy(i):
        return push(snd.at[i], d2d.at[i], d2d_sem.at[0, i], d2d_sem.at[1, i], {"tp": near})

    def x_copy(i):
        return push(xsnd.at[i], xrcv.at[i], x_sem.at[0, i], x_sem.at[1, i], {"tp": far})

    def ret_copy(r):
        return push(gsnd.at[r], grcv.at[r], ret_sem.at[0, r], ret_sem.at[1, r], {"sp": host})

    def put(h, block):
        out_ref[:, pl.ds(pl.multiple_of(h * feats, feats), feats)] = block

    def active(i):
        vals = CELLS[i]
        if all(v >= 0 for v in vals):
            return lambda body: body()
        return pl.when(pick(vals) >= 0)

    def kinds(i, own, guest):
        code = pick(CELLS[i])
        if all(v < n for v in CELLS[i]):
            own(code)
        else:
            if any(0 <= v < n for v in CELLS[i]):
                pl.when(code < n)(lambda: own(code))
            pl.when(code >= n)(lambda: guest(code % n, code // n - 1))

    def first(i):
        @active(i)
        def _():
            def own(j):
                return None

            def visitor(j, r):
                @pl.when(r == 0)
                def _():
                    act_copy(1).wait_recv()
                    act_copy(0).wait_recv()

            kinds(i, own, visitor)
            code = pick(CELLS[i])
            j = code % n
            if all(v < n for v in CELLS[i]):
                a, b = acts.at[0, 0], acts.at[0, 1]
            else:
                who = jnp.minimum(code // n, 1)
                a, b = acts.at[who, 0], acts.at[who, 1]
            share = lax.dot_general(a[...], wo[j, 0], NT, preferred_element_type=F32)
            share = (share + lax.dot_general(b[...], wo[j, 1], NT, preferred_element_type=F32)).astype(BF16)
            snd[i] = share[2 * rows :]
            keep[i] = share[: 2 * rows]
            d2d_copy(i).start()

    def second(i):
        @active(i)
        def _():
            d2d_copy(i).wait_recv()
            xsnd[i] = (keep[i, pl.ds(rows, rows)].astype(F32) + d2d[i, pl.ds(rows, rows)].astype(F32)).astype(BF16)
            x_copy(i).start()

    def third(i):
        @active(i)
        def _():
            x_copy(i).wait_recv()
            own = keep[i, pl.ds(0, rows)].astype(F32) + d2d[i, pl.ds(0, rows)].astype(F32)
            done = (own + xrcv[i].astype(F32)).astype(BF16)

            def visitor(j, r):
                gsnd[r] = done
                ret_copy(r).start()

            kinds(i, lambda j: put(j, done), visitor)

    steps = len(CELLS)
    for i in range(steps):
        pump(23 + i)
        first(i)
        if i >= 1:
            second(i - 1)
        if i >= 3:
            third(i - 3)
    second(steps - 1)
    for i in range(steps - 3, steps):
        third(i)
    pump(23 + steps)
    for r in range(len(CELL_BACK)):
        @pl.when(pick(CELL_BACK[r]) >= 0)
        def _():
            ret_copy(r).wait_recv()
            put(pick(CELL_BACK[r]), grcv[r])

    for copy in (*to_far, to_near, *relay):
        copy.wait_send()
    guard(sp < n - 1)(halo.wait_send)
    for point in range(len(EVENTS)):
        events(point, False, lambda copy: copy.wait_send())

    @pl.when(outer)
    def _():
        for i in range(2):
            act_copy(i).wait_send()

    for i in range(steps):
        @active(i)
        def _():
            d2d_copy(i).wait_send()
            x_copy(i).wait_send()
            kinds(i, lambda j: None, lambda j, r: ret_copy(r).wait_send())


def finish_kernel(out_ref, logw_ref, out, logw):
    out[...] = out_ref[...]
    logw[...] = logw_ref[...]


def finish(out, logw):
    vmem = pl.BlockSpec(memory_space=pltpu.VMEM)
    out, logw = pl.pallas_call(
        finish_kernel,
        out_shape=(jax.ShapeDtypeStruct(out.shape, out.dtype), jax.ShapeDtypeStruct(logw.shape, logw.dtype)),
        in_specs=[vmem, vmem],
        out_specs=(vmem, vmem),
    )(out, logw)
    return (out, logw.T)


def grid_local(
    n, tokens, norm_gain, w_query, w_key, w_value, score_shift, w_conv_b, w_conv_c, w_conv_u,
    conv_kernel, w_out_att, w_out_conv,
):
    rows, d = tokens.shape
    toks = 4 * rows
    feats, att_cols = w_out_att.shape
    conv_cols = w_out_conv.shape[1]
    heads = score_shift.shape[0]
    kv_cols = w_key.shape[1]
    cells = len(CELLS)
    guests = len(CELL_BACK)
    vmem = pl.BlockSpec(memory_space=pltpu.VMEM)
    hbm = pl.BlockSpec(memory_space=pl.ANY)
    dma = pltpu.SemaphoreType.DMA
    regular = pltpu.SemaphoreType.REGULAR
    out, logw = pl.pallas_call(
        functools.partial(grid_kernel, n),
        out_shape=(
            jax.ShapeDtypeStruct((rows, n * feats), BF16),
            jax.ShapeDtypeStruct((heads, toks), F32),
        ),
        in_specs=[hbm] * 12,
        out_specs=(vmem, vmem),
        scratch_shapes=[
            pltpu.VMEM((1, d), F32),
            pltpu.VMEM((1, heads), F32),
            pltpu.VMEM(conv_kernel.shape, F32),
            pltpu.VMEM(w_query.shape, BF16),
            pltpu.VMEM((d, 2 * kv_cols), BF16),
            *[pltpu.VMEM(w.shape, BF16) for w in (w_conv_b, w_conv_c, w_conv_u)],
            pltpu.VMEM((4, rows, d), BF16),
            pltpu.VMEM((2 * rows, d), BF16),
            pltpu.VMEM((heads * toks, HEAD_DIM), BF16),
            pltpu.VMEM((n, 2, 2, 2 * rows, kv_cols), BF16),
            pltpu.VMEM((n, 2, feats, att_cols), BF16),
            pltpu.VMEM((toks, conv_cols), BF16),
            pltpu.VMEM((toks, conv_cols), BF16),
            pltpu.VMEM((HALO, conv_cols), BF16),
            pltpu.VMEM((toks + HALO, conv_cols), F32),
            pltpu.VMEM((2, 2, toks, att_cols), BF16),
            *[pltpu.VMEM((heads * toks, HEAD_DIM), F32)] * 2,
            *[pltpu.VMEM((cells, 2 * rows, feats), BF16)] * 3,
            *[pltpu.VMEM((cells, rows, feats), BF16)] * 2,
            *[pltpu.VMEM((guests, rows, feats), BF16)] * 2,
            dma((13,)), dma((5,)), dma((5,)), dma((3, n, 3)), dma((n, 3)), dma((3, n, 4)), dma((n, 4)),
            dma((2,)), dma((2, cells)), dma((2, cells)), dma((2, 2)), dma((2, guests)), regular,
        ],
        compiler_params=pltpu.CompilerParams(
            collective_id=0, has_side_effects=True, vmem_limit_bytes=60 * 1024 * 1024
        ),
    )(
        tokens, norm_gain.reshape(1, d), w_query, w_key, w_value, score_shift.reshape(1, heads),
        w_conv_b, w_conv_c, w_conv_u, conv_kernel, w_out_att, w_out_conv,
    )
    return finish(out, logw)


def solution(mesh):
    n = mesh.shape["sp"]
    body = grid_local if n == len(CELLS[0]) and mesh.shape["tp"] == 4 else local
    return jax.shard_map(
        functools.partial(body, n),
        mesh=mesh,
        in_specs=(
            P(("sp", "tp"), None), P(), P(None, "tp"), P(None, "tp"), P(None, "tp"), P("tp"),
            P(None, "tp"), P(None, "tp"), P(None, "tp"), P(None, "tp"), P("sp", "tp"), P("sp", "tp"),
        ),
        out_specs=(P(("sp", "tp"), None), P("sp", "tp")),
        check_vma=False,
    )
```

```python
import functools

import jax
import jax.numpy as jnp
from jax import lax
from jax.experimental import pallas as pl
from jax.experimental.pallas import tpu as pltpu
from jax.sharding import PartitionSpec as P

HEAD_DIM = 128
CONV_K = 3
HALO = 16
F32 = jnp.float32
BF16 = jnp.bfloat16
MESH = pl.DeviceIdType.MESH
NT = (((1,), (1,)), ((), ()))
EVENTS = [[(8, 18), (136, 146), (266, 276), (398,), (518, 536), (648, 662), (780,), (908,)],
 [(74, 24, 34),
  (194, 152, 162),
  (330, 274, 292, 312),
  (450, 410, 420),
  (586, 530, 548, 568),
  (706, 686),
  (840, 792, 820),
  (920, 932)],
 [(), (), (), (), (), (), (), ()],
 [(), (), (), (), (), (), (), ()],
 [(), (184,), (308,), (436,), (), (692,), (), (956,)],
 [(), (), (), (), (), (), (), ()],
 [(40, 50),
  (178,),
  (290, 521, 75, 389),
  (418, 203, 261),
  (546, 265, 645, 331),
  (690, 905, 459, 533),
  (808, 585),
  (713, 773)],
 [(90, 56, 131), (210, 3, 425), (346,), (466,), (602, 821), (722, 937), (856, 917), (665,)],
 [(297,),
  (441,),
  (405, 306, 553, 645),
  (661, 434, 169, 697, 677),
  (562, 281),
  (900, 387, 409, 932),
  (521,),
  (789, 681)],
 [(106, 419),
  (226, 35, 265),
  (91, 362),
  (219, 482),
  (75, 347, 618, 917),
  (203, 475, 738),
  (329, 601, 872),
  (457, 729, 805)],
 [(), (), (), (), (), (), (), ()],
 [(), (), (825,), (185,), (), (), (661,), ()],
 [(), (), (), (), (), (), (), ()],
 [(313,), (), (165,), (517,), (933,), (565,), (), ()],
 [(), (665,), (), (), (920,), (793,), (537,), (697,)],
 [(), (), (), (), (), (), (), ()],
 [(),
  (291, 681, 65, 81, 97),
  (107, 19, 137, 693, 35, 917, 51, 193, 209, 225),
  (235, 147, 533, 321, 337, 353),
  (91, 363, 107, 642, 661, 313, 291, 789, 25, 449, 465, 481),
  (219, 949, 491, 235, 259, 577, 593, 609),
  (73, 345, 617, 89, 361, 105, 693, 553, 705, 721, 737),
  (517, 201, 473, 745, 833, 849, 865)],
 [(), (), (), (178, 9), (930,), (), (), (217,)],
 [(),
  (),
  (),
  (901, 2, 569, 65, 81, 97),
  (193, 209, 225),
  (419, 773, 809, 277, 153, 321, 337, 353),
  (569, 449, 465, 481),
  (489, 233, 393, 577, 593, 609)],
 [(), (), (), (), (), (274,), (), ()],
 [(), (), (), (), (), (65, 81, 97), (193, 209, 225), (265, 321, 337, 353)],
 [(), (), (), (), (), (), (649,), ()],
 [(), (), (), (), (), (), (), (65, 81, 97)],
 [(), (), (162, 933), (), (403, 41, 805), (435, 804, 185), (), (425,)],
 [(385, 401, 433), (17, 49), (1,), (549,), (), (), (), (281, 529, 545, 561)],
 [(408, 257, 273),
  (521, 537, 385, 401),
  (130, 793, 565, 417, 433),
  (546, 953, 129),
  (306, 57, 673, 689),
  (913,),
  (297, 389, 673),
  (441, 641)],
 [(649, 434, 145, 161, 177),
  (905, 643, 553, 689),
  (434, 949, 657, 673),
  (933, 819, 777, 948, 130, 273, 289, 305),
  (149, 769),
  (916, 307, 9, 513, 545),
  (897, 929, 945),
  (289, 305)],
 [(697, 675, 657),
  (913, 929, 945),
  (946, 769, 801),
  (641,),
  (169, 129, 177),
  (21, 819),
  (409, 421, 257, 273, 305),
  (817,)],
 [(921, 531, 569, 899, 929, 945), (561,), (), (276, 290, 785, 801), (1,), (53, 33), (433,), (401,)],
 [(513, 545), (273, 305), (529,), (), (), (), (), ()],
 [(), (), (145, 177), (913,), (), (129, 161), (), ()],
 [(), (), (897,), (17, 33, 49), (897, 945), (), (), ()],
 [(), (), (), (), (385, 417, 433), (289,), (), ()],
 [(), (), (), (), (), (), (), ()]]
CELLS = [(0, 1, 2, 3, 4, 5, 6, 7),
 (3, 0, 0, 4, 2, 3, 4, 4),
 (2, 3, 3, 1, 5, 7, 5, 5),
 (1, 5, 5, 2, 6, 4, 7, 2),
 (5, 7, 14, 5, 1, 6, 2, 6),
 (7, 4, 6, 14, 0, 8, 3, 3),
 (4, 2, 4, 6, 8, 0, -1, -1),
 (-1, -1, 1, 7, 17, 17, -1, -1),
 (-1, -1, 7, 0, 7, 1, -1, -1),
 (-1, -1, -1, -1, 3, 2, -1, -1)]
CELL_BACK = [(6, 6, -1, -1, -1, -1, 0, 0), (-1, -1, -1, -1, -1, -1, 1, 1)]


def softplus(z):
    u = jnp.exp(-jnp.abs(z))
    small = u * (1.0 - u * (0.5 - u * (1.0 / 3.0 - u * 0.25)))
    return jnp.maximum(z, 0.0) + jnp.where(u < 0.01, small, jnp.log(1.0 + u))


def kernel(
    n,
    tok_ref, gain_ref, wq_hbm, wk_hbm, wv_hbm, shift_ref, wb_hbm, wc_hbm, wu_hbm, taps_ref, woa_ref, woc_ref,
    out_ref, logw_ref,
    wq, wk, wv, wb, wc, wu, xall, normed, q_sc, kv, wo, gate_sc, prod_sc, prev, ext, attn, conv, partial, totals,
    snd, keep, d2d, xsnd, xrcv,
    load_sem, tok_ssem, tok_rsem, kv_sem, w_sem, halo_sem, d2d_sem, x_sem,
):
    sp = lax.axis_index("sp")
    t = lax.axis_index("tp")
    near = t + 1 - 2 * (t % 2)
    far = t + 2 - 4 * ((t // 2) % 2)
    diag = near + 2 - 4 * ((near // 2) % 2)
    pos = jnp.where(sp % 2 == 0, sp // 2, n - 1 - sp // 2)

    def ring(place):
        place = (place + 2 * n) % n
        return jnp.where(place < n // 2, 2 * place, 2 * (n - 1 - place) + 1)

    right, left = ring(pos + 1), ring(pos - 1)
    following, leading = (sp + 1) % n, (sp + n - 1) % n
    rows = tok_ref.shape[0]
    toks = 4 * rows
    half = rows // 2
    fpart = wo.shape[2] // 2
    heads = q_sc.shape[1] // HEAD_DIM
    kv_cols = kv.shape[4]
    grouping = heads // (kv_cols // HEAD_DIM)

    loads = [
        pltpu.make_async_copy(src, dst, load_sem.at[i])
        for i, (src, dst) in enumerate(
            ((wk_hbm, wk), (wv_hbm, wv), (wq_hbm, wq), (wc_hbm, wc), (wu_hbm, wu), (wb_hbm, wb))
        )
    ]
    own_loads = [
        pltpu.make_async_copy(src, wo.at[sp, i], load_sem.at[6 + i]) for i, src in enumerate((woa_ref, woc_ref))
    ]
    barrier = pltpu.get_barrier_semaphore()
    for place in (right, left, following, leading):
        pl.semaphore_signal(barrier, inc=1, device_id={"sp": place}, device_id_type=MESH)
    for place in (near, far):
        pl.semaphore_signal(barrier, inc=1, device_id={"tp": place}, device_id_type=MESH)
    for load in (*own_loads, *loads):
        load.start()
    pl.semaphore_wait(barrier, 6)

    def push(src, dst, ssem, rsem, who):
        return pltpu.make_async_remote_copy(
            src_ref=src, dst_ref=dst, send_sem=ssem, recv_sem=rsem, device_id=who, device_id_type=MESH
        )

    to_far = [
        push(tok_ref.at[pl.ds(c * half, half)], xall.at[t, pl.ds(c * half, half)], tok_ssem.at[c], tok_rsem.at[c], {"tp": far})
        for c in range(2)
    ]
    to_near = push(tok_ref, xall.at[t], tok_ssem.at[2], tok_rsem.at[2], {"tp": near})
    relay = [
        push(xall.at[far, pl.ds(c * half, half)], xall.at[far, pl.ds(c * half, half)], tok_ssem.at[3 + c], tok_rsem.at[3 + c], {"tp": near})
        for c in range(2)
    ]
    for copy in to_far:
        copy.start()
    to_near.start()

    last = n // 2

    def hop(part, sem, way, step, chunk):
        block = ring(pos - (step - 1)) if way == 0 else ring(pos + (step - 1))
        view = part(block, chunk, step)
        return push(
            view[0], view[1], sem.at[0, way, step - 1, chunk], sem.at[1, way, step - 1, chunk],
            {"sp": right if way == 0 else left},
        )

    def ways(step, chunk, chunks):
        if isinstance(step, int) and step == last:
            return (0,) if chunk < chunks // 2 else (1,)
        return (0, 1)

    early = t // 2

    def kv_part(block, chunk, step):
        view = kv.at[block, early + chunk * (1 - 2 * early)]
        return view, view

    def w_part(block, chunk, step):
        view = wo.at[block, chunk // 2, pl.ds(pl.multiple_of((chunk % 2) * fpart, fpart), fpart)]
        return view, view

    rings = {"kv": (kv_part, kv_sem, 2), "w": (w_part, w_sem, 4)}

    def emit(name, step, chunk):
        part, sem, chunks = rings[name]
        for way in ways(step, chunk, chunks):
            hop(part, sem, way, step, chunk).start()

    def take(name, step, chunk, onward=None):
        part, sem, chunks = rings[name]
        for way in ways(step, chunk, chunks):
            hop(part, sem, way, step, chunk).wait_recv()
        if onward or (onward is None and step < last):
            emit(name, step + 1, chunk)

    for load in own_loads:
        load.wait()
    for chunk in (0, 1):
        emit("w", 1, chunk)

    def dot(w):
        return jnp.dot(normed[...], w[...], preferred_element_type=F32).astype(BF16)

    def project_kv(groups, pair):
        for i, g in enumerate(groups):
            x = (tok_ref[...] if g is None else xall[g]).astype(F32)
            inverse = lax.rsqrt(jnp.mean(x * x, axis=-1, keepdims=True) + 1e-06)
            at = rows * (t % 2 if i == 0 else 1 - t % 2)
            normed[pl.ds(pl.multiple_of(at, rows), rows)] = (x * inverse * gain_ref[...]).astype(BF16)
        kv[sp, pair, 0] = dot(wk)
        kv[sp, pair, 1] = dot(wv)

    def project_rest(pair):
        at = pl.ds(pl.multiple_of(pair * 2 * rows, 2 * rows), 2 * rows)
        prod_sc[at] = (dot(wc).astype(F32) * dot(wu).astype(F32)).astype(BF16)
        q_sc[at] = dot(wq)
        gate_sc[at] = dot(wb)

    to_near.wait_recv()
    for load in loads[:2]:
        load.wait()
    project_kv((None, near), early)
    emit("kv", 1, 0)
    for chunk in (2, 3):
        emit("w", 1, chunk)
    for load in loads[2:]:
        load.wait()
    project_rest(early)
    to_far[0].wait_recv()
    relay[0].start()
    take("kv", 1, 0)
    take("w", 1, 0)
    to_far[1].wait_recv()
    relay[1].start()
    for c in range(2):
        relay[c].wait_recv()
    project_kv((far, diag), 1 - early)
    emit("kv", 1, 1)
    take("w", 1, 1)
    take("w", 1, 2)
    project_rest(1 - early)
    halo = push(prod_sc.at[pl.ds(toks - HALO, HALO)], prev, halo_sem.at[0], halo_sem.at[1], {"sp": following})
    halo.start()

    key_i = lax.broadcasted_iota(jnp.int32, (toks, toks), 0)
    key_j = lax.broadcasted_iota(jnp.int32, (toks, toks), 1)
    later = (key_i > key_j).astype(F32).astype(BF16)
    lane = lax.broadcasted_iota(jnp.int32, (toks, totals.shape[2]), 1)
    scale = HEAD_DIM ** (-0.5)
    order = (t, far, near, diag)

    def visit(slot, masked):
        for h in range(heads):
            cols = pl.ds(h * HEAD_DIM, HEAD_DIM)
            kv_at = pl.ds((h // grouping) * HEAD_DIM, HEAD_DIM)
            keys = kv[slot, :, 0, :, kv_at].reshape(toks, HEAD_DIM)
            vals = kv[slot, :, 1, :, kv_at].reshape(toks, HEAD_DIM)
            z = lax.dot_general(q_sc[:, cols], keys, NT, preferred_element_type=F32) * scale + shift_ref[0, h]
            soft = softplus(z)
            if masked:
                soft = jnp.where(key_j < key_i, soft, 0.0)
            high = soft.astype(BF16)
            low = (soft - high.astype(F32)).astype(BF16)
            after = jnp.dot(high, later, preferred_element_type=F32) + jnp.dot(low, later, preferred_element_type=F32)
            weight = jnp.exp(z - soft - after)
            if masked:
                weight = jnp.where(key_j < key_i, weight, 0.0)
            partial[slot, :, cols] = jnp.dot(weight.astype(BF16), vals, preferred_element_type=F32)
            total = after[:, 0:1] + soft[:, 0:1]
            totals[h] = jnp.where(lane == slot, total, totals[h])

    def visit_at(step, both=True):
        def side(i, carry):
            slot = ring(pos + (2 * i - 1) * step)

            @pl.when(slot < sp)
            def _():
                visit(slot, False)

            return carry

        lax.fori_loop(0, 2 if both else 1, side, 0)

    totals[...] = jnp.zeros(totals.shape, F32)
    visit(sp, True)

    def w_event(m):
        return m // 4 + 1, m % 4

    def body(s, carry):
        if n > 4:
            take("kv", s + 1, 0, True)
            take("kv", s, 1, True)
            take("w", *w_event(2 * s + 1), True)
            take("w", *w_event(2 * s + 2), True)
            visit_at(s)
        return carry

    def convolve():
        halo.wait_recv()
        ext[pl.ds(HALO, toks)] = prod_sc[...].astype(F32)
        ext[pl.ds(0, HALO)] = jnp.where(sp == 0, 0.0, prev[...].astype(F32))
        summed = jnp.zeros((toks, ext.shape[1]), F32)
        for tap in range(CONV_K):
            summed = summed + taps_ref[tap : tap + 1, :] * ext[pl.ds(HALO - (CONV_K - 1) + tap, toks)]
        ext[pl.ds(HALO, toks)] = gate_sc[...].astype(F32) * summed
        for i, g in enumerate(order):
            conv[pl.ds(i * rows, rows)] = ext[pl.ds(pl.multiple_of(HALO + g * rows, HALO), rows)].astype(BF16)

    loops = max(last - 3, 0)
    lax.fori_loop(1, 1 + loops, body, 0)
    w_done = 3 + 2 * loops
    convolve()
    for s in range(1 + loops, last + 1):
        if s + 1 <= last:
            take("kv", s + 1, 0)
        take("kv", s, 1)
        for m in range(w_done, w_done + 2 if s < last else w_done + 1):
            take("w", *w_event(m))
            w_done += 1
        visit_at(s, s < last)

    def combine(i, carry):
        slot = sp - i
        suffixes = []
        for h in range(heads):
            cols = pl.ds(h * HEAD_DIM, HEAD_DIM)
            suffix = carry[h]
            ext[pl.ds(HALO, toks), cols] += jnp.exp(-suffix) * partial[slot, :, cols]
            total = jnp.sum(jnp.where(lane == slot, totals[h], 0.0), axis=1, keepdims=True)
            suffixes.append(suffix + total)
        return tuple(suffixes)

    ext[...] = jnp.zeros(ext.shape, F32)
    suffixes = lax.fori_loop(0, sp + 1, combine, tuple(jnp.zeros((toks, 1), F32) for _ in range(heads)))
    for h in range(heads):
        spread = jnp.broadcast_to(suffixes[h], (toks, 128)).T[0:1, :]
        logw_ref[h : h + 1, :] = jnp.log(jnp.maximum(1.0 - jnp.exp(-spread), 0.05))
    for i, g in enumerate(order):
        attn[pl.ds(i * rows, rows)] = ext[pl.ds(pl.multiple_of(HALO + g * rows, HALO), rows), 0 : attn.shape[1]].astype(BF16)

    def block_of(i):
        return ring(pos - (i + 1) // 2) if i % 2 else ring(pos + i // 2)

    def d2d_copy(i):
        return push(snd.at[i], d2d.at[i], d2d_sem.at[0, i], d2d_sem.at[1, i], {"tp": near})

    def x_copy(i):
        return push(xsnd.at[i], xrcv.at[i], x_sem.at[0, i], x_sem.at[1, i], {"tp": far})

    def first(i):
        j = block_of(i)
        share = lax.dot_general(attn[...], wo[j, 0], NT, preferred_element_type=F32)
        share = (share + lax.dot_general(conv[...], wo[j, 1], NT, preferred_element_type=F32)).astype(BF16)
        snd[i] = share[2 * rows :]
        keep[i] = share[: 2 * rows]
        d2d_copy(i).start()

    def second(i):
        d2d_copy(i).wait_recv()
        xsnd[i] = (keep[i, pl.ds(rows, rows)].astype(F32) + d2d[i, pl.ds(rows, rows)].astype(F32)).astype(BF16)
        x_copy(i).start()

    def third(i):
        x_copy(i).wait_recv()
        own = keep[i, pl.ds(0, rows)].astype(F32) + d2d[i, pl.ds(0, rows)].astype(F32)
        done = (own + xrcv[i].astype(F32)).astype(BF16)
        if len(out_ref.shape) == 3:
            out_ref[block_of(i)] = done
        else:
            feats = keep.shape[2]
            out_ref[:, pl.ds(pl.multiple_of(block_of(i) * feats, feats), feats)] = done

    for i in range(n):
        while w_done < max(4 * ((i + 1) // 2), min(10 + i, 4 * last)):
            take("w", *w_event(w_done))
            w_done += 1
        first(i)
        if i >= 1:
            second(i - 1)
        if i >= 3:
            third(i - 3)
    second(n - 1)
    for i in range(max(n - 3, 0), n):
        third(i)

    for copy in (*to_far, to_near, *relay, halo):
        copy.wait_send()
    for part, sem, chunks in rings.values():
        for step in range(1, last + 1):
            for chunk in range(chunks):
                for way in ways(step, chunk, chunks):
                    hop(part, sem, way, step, chunk).wait_send()
    for i in range(n):
        d2d_copy(i).wait_send()
        x_copy(i).wait_send()


def local(
    n, tokens, norm_gain, w_query, w_key, w_value, score_shift, w_conv_b, w_conv_c, w_conv_u,
    conv_kernel, w_out_att, w_out_conv,
):
    rows, d = tokens.shape
    toks = 4 * rows
    feats, att_cols = w_out_att.shape
    conv_cols = w_out_conv.shape[1]
    heads = score_shift.shape[0]
    kv_cols = w_key.shape[1]
    vmem = pl.BlockSpec(memory_space=pltpu.VMEM)
    smem = pl.BlockSpec(memory_space=pltpu.SMEM)
    hbm = pl.BlockSpec(memory_space=pl.ANY)
    dma = pltpu.SemaphoreType.DMA
    wide = feats % 128 == 0
    out, logw = pl.pallas_call(
        functools.partial(kernel, n),
        out_shape=(
            jax.ShapeDtypeStruct((rows, n * feats) if wide else (n, rows, feats), BF16),
            jax.ShapeDtypeStruct((heads, toks), F32),
        ),
        in_specs=[vmem, vmem, hbm, hbm, hbm, smem, hbm, hbm, hbm, vmem, hbm, hbm],
        out_specs=(vmem, vmem),
        scratch_shapes=[
            *[pltpu.VMEM(w.shape, BF16) for w in (w_query, w_key, w_value, w_conv_b, w_conv_c, w_conv_u)],
            pltpu.VMEM((4, rows, d), BF16),
            pltpu.VMEM((2 * rows, d), BF16),
            pltpu.VMEM((toks, w_query.shape[1]), BF16),
            pltpu.VMEM((n, 2, 2, 2 * rows, kv_cols), BF16),
            pltpu.VMEM((n, 2, feats, att_cols), BF16),
            pltpu.VMEM((toks, conv_cols), BF16),
            pltpu.VMEM((toks, conv_cols), BF16),
            pltpu.VMEM((HALO, conv_cols), BF16),
            pltpu.VMEM((toks + HALO, max(conv_cols, att_cols)), F32),
            pltpu.VMEM((toks, att_cols), BF16),
            pltpu.VMEM((toks, conv_cols), BF16),
            pltpu.VMEM((n, toks, att_cols), F32),
            pltpu.VMEM((heads, toks, 128), F32),
            pltpu.VMEM((n, 2 * rows, feats), BF16),
            pltpu.VMEM((n, 2 * rows, feats), BF16),
            pltpu.VMEM((n, 2 * rows, feats), BF16),
            pltpu.VMEM((n, rows, feats), BF16),
            pltpu.VMEM((n, rows, feats), BF16),
            dma((8,)), dma((5,)), dma((5,)), dma((2, 2, n // 2, 2)), dma((2, 2, n // 2, 4)), dma((2,)), dma((2, n)), dma((2, n)),
        ],
        compiler_params=pltpu.CompilerParams(
            collective_id=0, has_side_effects=True, vmem_limit_bytes=60 * 1024 * 1024
        ),
    )(
        tokens, norm_gain.reshape(1, d), w_query, w_key, w_value, score_shift.reshape(1, heads),
        w_conv_b, w_conv_c, w_conv_u, conv_kernel, w_out_att, w_out_conv,
    )
    if not wide:
        out = out.transpose(1, 0, 2).reshape(rows, n * feats)
    return (out, logw.T)

def soft_plus(z):
    u = jnp.exp(-jnp.abs(z))
    small = u - (u * u) * (0.5 - u * (1.0 / 3.0))
    return jnp.maximum(z, 0.0) + jnp.where(u < 0.005, small, jnp.log(1.0 + u))


def grid_kernel(
    n,
    tok_hbm, gain_hbm, wq_hbm, wk_hbm, wv_hbm, shift_hbm, wb_hbm, wc_hbm, wu_hbm, taps_hbm, woa_ref, woc_ref,
    out_ref, logw_ref,
    gain_ref, shift_ref, taps_ref, wq, wkv, wb, wc, wu, xall, normed, q_sc, kv, wo, gate_sc, prod_sc, prev, ext, acts, acc, suffix,
    snd, keep, d2d, xsnd, xrcv, gsnd, grcv,
    load_sem, tok_ssem, tok_rsem, kv_ssem, kv_rsem, w_ssem, w_rsem, halo_sem, d2d_sem, x_sem,
    act_sem, ret_sem, near_by,
):
    sp = lax.axis_index("sp")
    t = lax.axis_index("tp")
    z = sp // 2
    y = sp % 2
    near = t + 1 - 2 * (t % 2)
    far = t + 2 - 4 * ((t // 2) % 2)
    diag = near + 2 - 4 * ((near // 2) % 2)
    up, down, side = sp + 2, sp - 2, sp + 1 - 2 * y
    ways = (up, down, side)
    host = sp + 2 - 4 * (z % 2)
    levels = n // 2
    has_up, has_down = z < levels - 1, z > 0
    outer = jnp.logical_or(z == 0, z == levels - 1)
    rows = tok_hbm.shape[0]
    toks = 4 * rows
    half = rows // 2
    fpart = wo.shape[2] // 2
    feats = wo.shape[2]
    heads = q_sc.shape[0] // toks
    kv_cols = kv.shape[4]
    grouping = heads // (kv_cols // HEAD_DIM)

    def pick(vals):
        out = vals[0]
        for i in range(1, n):
            if vals[i] != vals[0] or not isinstance(out, int):
                out = jnp.where(sp == i, vals[i], out)
        return out

    def guard(cond):
        return pl.when(cond)

    loads = [
        pltpu.make_async_copy(src, dst, load_sem.at[i])
        for i, (src, dst) in enumerate(
            (
                (wk_hbm, wkv.at[:, pl.ds(0, kv_cols)]), (wv_hbm, wkv.at[:, pl.ds(kv_cols, kv_cols)]),
                (wc_hbm, wc), (wu_hbm, wu), (wq_hbm, wq), (wb_hbm, wb),
            )
        )
    ]
    own_loads = [
        pltpu.make_async_copy(src, wo.at[sp, i], load_sem.at[6 + i]) for i, src in enumerate((woa_ref, woc_ref))
    ]
    tok_loads = [
        pltpu.make_async_copy(tok_hbm.at[pl.ds(c * half, half)], xall.at[t, pl.ds(c * half, half)], load_sem.at[8 + c])
        for c in range(2)
    ]
    small_loads = [
        pltpu.make_async_copy(src, dst, load_sem.at[10 + i])
        for i, (src, dst) in enumerate(((gain_hbm, gain_ref), (shift_hbm, shift_ref), (taps_hbm, taps_ref)))
    ]
    barrier = pltpu.get_barrier_semaphore()

    def tell(sem, place):
        pl.semaphore_signal(sem, inc=1, device_id={"sp": place}, device_id_type=MESH)

    def tell_column(sem):
        guard(has_up)(lambda: tell(sem, up))
        guard(has_down)(lambda: tell(sem, down))

    column = has_up.astype(jnp.int32) + has_down.astype(jnp.int32)
    for place in (near, far):
        pl.semaphore_signal(barrier, inc=1, device_id={"tp": place}, device_id_type=MESH)
    tell(barrier, side)
    tell_column(barrier)
    for load in (*tok_loads, *own_loads, *small_loads, *loads):
        load.start()
    pl.semaphore_wait(barrier, 3 + column)

    def push(src, dst, ssem, rsem, who):
        return pltpu.make_async_remote_copy(
            src_ref=src, dst_ref=dst, send_sem=ssem, recv_sem=rsem, device_id=who, device_id_type=MESH
        )

    to_far = [
        push(xall.at[t, pl.ds(c * half, half)], xall.at[t, pl.ds(c * half, half)], tok_ssem.at[c], tok_rsem.at[c], {"tp": far})
        for c in range(2)
    ]
    to_near = push(xall.at[t], xall.at[t], tok_ssem.at[2], tok_rsem.at[2], {"tp": near})
    relay = [
        push(xall.at[far, pl.ds(c * half, half)], xall.at[far, pl.ds(c * half, half)], tok_ssem.at[3 + c], tok_rsem.at[3 + c], {"tp": near})
        for c in range(2)
    ]
    for load, copy in zip(tok_loads, to_far):
        load.wait()
        copy.start()
    to_near.start()
    tell_column(near_by)

    early = t // 2

    def hop_copy(site, h, c, d):
        if c < 4:
            view = wo.at[h, c // 2, pl.ds(c % 2 * fpart, fpart)]
            sems = (w_ssem.at[d, h, c], w_rsem.at[h, c])
        else:
            view = kv.at[h, early] if c == 4 else kv.at[h, 1 - early, :, pl.ds((c - 5) * rows, rows)]
            sems = (kv_ssem.at[d, h, c - 4], kv_rsem.at[h, c - 4])
        return push(view, view, *sems, {"sp": (site + 2, site - 2, site ^ 1)[d]})

    def at_site(bodies, low=0, high=n):
        if all(body is None for body in bodies[low:high]):
            return
        if high - low == 1:
            bodies[low]()
            return
        mid = (low + high) // 2
        lax.cond(sp < mid, lambda: at_site(bodies, low, mid), lambda: at_site(bodies, mid, high))

    def events(lists, arrive, leave):
        def body_of(site, codes):
            def body():
                for code in codes:
                    h, c = code // 128, code // 16 % 8
                    if arrive and code % 2:
                        hop_copy(site, h, c, 2).wait_recv()
                    for d in range(3):
                        if code // 2 // 2**d % 2:
                            leave(hop_copy(site, h, c, d))

            return body if codes else None

        at_site([body_of(site, codes) for site, codes in enumerate(lists)])

    def pump(point):
        events(EVENTS[point], True, lambda copy: copy.start())

    def drain(first_point, last_point):
        merged = [
            tuple(code for point in EVENTS[first_point:last_point] for code in point[site]) for site in range(n)
        ]
        events(merged, False, lambda copy: copy.wait_send())

    for load in own_loads:
        load.wait()
    pump(0)
    for load in small_loads:
        load.wait()

    def dot(w):
        return jnp.dot(normed[...], w[...], preferred_element_type=F32)

    def normalize(g, same, low, count):
        x = xall[g, pl.ds(low, count)].astype(F32)
        inverse = lax.rsqrt(jnp.mean(x * x, axis=-1, keepdims=True) + 1e-06)
        at = rows * (t % 2 if same else 1 - t % 2) + low
        normed[pl.ds(pl.multiple_of(at, half), count)] = (x * inverse * gain_ref[...]).astype(BF16)

    def project_early():
        normalize(t, True, 0, rows)
        normalize(near, False, 0, rows)
        both = dot(wkv).astype(BF16)
        kv[sp, early, 0] = both[:, :kv_cols]
        kv[sp, early, 1] = both[:, kv_cols:]

    def project_late(c):
        normalize(far, True, c * half, half)
        normalize(diag, False, c * half, half)
        some = jnp.concatenate([normed[pl.ds(c * half, half)], normed[pl.ds(rows + c * half, half)]], axis=0)
        both = jnp.dot(some, wkv[...], preferred_element_type=F32).astype(BF16)
        at = pl.ds(c * rows, rows)
        kv[sp, 1 - early, 0, at] = both[:, :kv_cols]
        kv[sp, 1 - early, 1, at] = both[:, kv_cols:]

    def project_rest(pair, points):
        at = pl.ds(pl.multiple_of(pair * 2 * rows, 2 * rows), 2 * rows)
        gate = dot(wc).astype(BF16).astype(F32)
        pump(points[0])
        prod_sc[at] = (gate * dot(wu).astype(BF16).astype(F32)).astype(BF16)
        pump(points[1])
        queries = dot(wq).astype(BF16)
        for h in range(heads):
            to = pl.ds(pl.multiple_of(h * toks + pair * 2 * rows, 2 * rows), 2 * rows)
            q_sc[to] = queries[:, h * HEAD_DIM : (h + 1) * HEAD_DIM]
        pump(points[2])
        gate_sc[at] = dot(wb).astype(BF16)
        pump(points[3])

    to_near.wait_recv()
    for load in loads[:2]:
        load.wait()
    project_early()
    pump(1)
    for load in loads[2:]:
        load.wait()
    project_rest(early, (2, 3, 4, 5))
    for c in range(2):
        pump(6 + 2 * c)
        to_far[c].wait_recv()
        relay[c].start()
        relay[c].wait_recv()
        project_late(c)
        pump(7 + 2 * c)
    project_rest(1 - early, (10, 11, 12, 13))
    pl.semaphore_wait(near_by, column)
    halo = push(prod_sc.at[pl.ds(toks - HALO, HALO)], prev, halo_sem.at[0], halo_sem.at[1], {"sp": sp + 1})
    guard(sp < n - 1)(halo.start)

    def spot(index):
        index = index % toks
        pair, sub = index // (2 * rows), index % (2 * rows)
        moved = sub % rows // half * rows + sub // rows * half + sub % half
        return jnp.where(pair == early, index, pair * 2 * rows + moved)

    later = spot(lax.broadcasted_iota(jnp.int32, (2 * toks, 1), 0)) > spot(lax.broadcasted_iota(jnp.int32, (1, toks), 1))
    later = later.astype(F32).astype(BF16)
    stacked = grouping * toks
    query = lax.broadcasted_iota(jnp.int32, (stacked, 1), 0) % toks
    causal = spot(lax.broadcasted_iota(jnp.int32, (1, toks), 1)) < query
    head_of = lax.broadcasted_iota(jnp.int32, (stacked, 1), 0) // toks
    scale = HEAD_DIM ** (-0.5)
    order = (t, far, near, diag)

    def visit(slot, masked):
        for g in range(heads // grouping):
            at = pl.ds(g * stacked, stacked)
            kv_at = pl.ds(g * HEAD_DIM, HEAD_DIM)
            keys = kv[slot, :, 0, :, kv_at].reshape(toks, HEAD_DIM)
            vals = kv[slot, :, 1, :, kv_at].reshape(toks, HEAD_DIM)
            shift = shift_ref[0:1, g * grouping : g * grouping + 1]
            for h in range(1, grouping):
                shift = jnp.where(head_of < h, shift, shift_ref[0:1, g * grouping + h : g * grouping + h + 1])
            s = lax.dot_general(q_sc[at], keys, NT, preferred_element_type=F32) * scale + shift
            soft = soft_plus(s)
            if masked:
                soft = jnp.where(causal, soft, 0.0)
            high = soft.astype(BF16)
            low = (soft - high.astype(F32)).astype(BF16)
            after = jnp.dot(jnp.concatenate([high, low], axis=1), later, preferred_element_type=F32)
            weight = jnp.exp(s - soft - after)
            if masked:
                weight = jnp.where(causal, weight, 0.0)
            part = jnp.dot(weight.astype(BF16), vals, preferred_element_type=F32)
            total = jnp.broadcast_to(after[:, 0:1] + soft[:, 0:1], (stacked, HEAD_DIM))
            if masked:
                acc[at] = part
                suffix[at] = total
            else:
                acc[at] += jnp.exp(-suffix[at]) * part
                suffix[at] += total

    def convolve():
        @pl.when(sp == 0)
        def _():
            prev[...] = jnp.zeros(prev.shape, BF16)

        guard(sp > 0)(halo.wait_recv)
        ext[pl.ds(HALO, toks)] = prod_sc[...].astype(F32)
        ext[pl.ds(0, HALO)] = prev[...].astype(F32)
        summed = jnp.zeros((toks, ext.shape[1]), F32)
        for tap in range(CONV_K):
            summed = summed + taps_ref[tap : tap + 1, :] * ext[pl.ds(HALO - (CONV_K - 1) + tap, toks)]
        ext[pl.ds(HALO, toks)] = gate_sc[...].astype(F32) * summed
        for i, g in enumerate(order):
            acts[0, 1, pl.ds(i * rows, rows)] = ext[pl.ds(pl.multiple_of(HALO + g * rows, HALO), rows)].astype(BF16)

    def act_copy(i):
        return push(acts.at[0, i], acts.at[1, i], act_sem.at[0, i], act_sem.at[1, i], {"sp": host})

    visit(sp, True)
    pump(14)
    convolve()
    guard(outer)(lambda: act_copy(1).start())
    pump(15)
    for i in range(1, n):
        pump(15 + i)

        @pl.when(sp >= i)
        def _():
            visit(sp - i, False)

    for h in range(heads):
        for i, g in enumerate(order):
            have = acc[pl.ds(pl.multiple_of(h * toks + g * rows, rows), rows)]
            acts[0, 0, pl.ds(i * rows, rows), pl.ds(h * HEAD_DIM, HEAD_DIM)] = have.astype(BF16)
    guard(outer)(lambda: act_copy(0).start())

    def d2d_copy(i):
        return push(snd.at[i], d2d.at[i], d2d_sem.at[0, i], d2d_sem.at[1, i], {"tp": near})

    def x_copy(i):
        return push(xsnd.at[i], xrcv.at[i], x_sem.at[0, i], x_sem.at[1, i], {"tp": far})

    def ret_copy(r):
        return push(gsnd.at[r], grcv.at[r], ret_sem.at[0, r], ret_sem.at[1, r], {"sp": host})

    def put(h, block):
        out_ref[:, pl.ds(pl.multiple_of(h * feats, feats), feats)] = block

    def active(i):
        vals = CELLS[i]
        if all(v >= 0 for v in vals):
            return lambda body: body()
        return pl.when(pick(vals) >= 0)

    def kinds(i, own, guest):
        code = pick(CELLS[i])
        if all(v < n for v in CELLS[i]):
            own(code)
        else:
            if any(0 <= v < n for v in CELLS[i]):
                pl.when(code < n)(lambda: own(code))
            pl.when(code >= n)(lambda: guest(code % n, code // n - 1))

    def first(i):
        @active(i)
        def _():
            def own(j):
                return None

            def visitor(j, r):
                @pl.when(r == 0)
                def _():
                    act_copy(1).wait_recv()
                    act_copy(0).wait_recv()

            kinds(i, own, visitor)
            code = pick(CELLS[i])
            j = code % n
            if all(v < n for v in CELLS[i]):
                a, b = acts.at[0, 0], acts.at[0, 1]
            else:
                who = jnp.minimum(code // n, 1)
                a, b = acts.at[who, 0], acts.at[who, 1]
            share = lax.dot_general(a[...], wo[j, 0], NT, preferred_element_type=F32)
            share = (share + lax.dot_general(b[...], wo[j, 1], NT, preferred_element_type=F32)).astype(BF16)
            snd[i] = share[2 * rows :]
            keep[i] = share[: 2 * rows]
            d2d_copy(i).start()

    def second(i):
        @active(i)
        def _():
            d2d_copy(i).wait_recv()
            xsnd[i] = (keep[i, pl.ds(rows, rows)].astype(F32) + d2d[i, pl.ds(rows, rows)].astype(F32)).astype(BF16)
            x_copy(i).start()

    def third(i):
        @active(i)
        def _():
            x_copy(i).wait_recv()
            own = keep[i, pl.ds(0, rows)].astype(F32) + d2d[i, pl.ds(0, rows)].astype(F32)
            done = (own + xrcv[i].astype(F32)).astype(BF16)

            def visitor(j, r):
                gsnd[r] = done
                ret_copy(r).start()

            kinds(i, lambda j: put(j, done), visitor)

    steps = len(CELLS)
    for i in range(steps):
        pump(23 + i)
        first(i)
        if i >= 1:
            second(i - 1)
        if i >= 3:
            third(i - 3)
    second(steps - 1)
    for h in range(heads):
        spread = suffix[pl.ds(h * toks, toks)].T[0:1, :]
        logw_ref[h : h + 1, :] = jnp.log(jnp.maximum(1.0 - jnp.exp(-spread), 0.05))
    for i in range(steps - 3, steps):
        third(i)
    pump(23 + steps)
    for r in range(len(CELL_BACK)):
        @pl.when(pick(CELL_BACK[r]) >= 0)
        def _():
            ret_copy(r).wait_recv()
            put(pick(CELL_BACK[r]), grcv[r])

    for copy in (*to_far, to_near, *relay):
        copy.wait_send()
    guard(sp < n - 1)(halo.wait_send)
    drain(0, len(EVENTS))

    @pl.when(outer)
    def _():
        for i in range(2):
            act_copy(i).wait_send()

    for i in range(steps):
        @active(i)
        def _():
            d2d_copy(i).wait_send()
            x_copy(i).wait_send()
            kinds(i, lambda j: None, lambda j, r: ret_copy(r).wait_send())


def finish_kernel(out_ref, logw_ref, out, logw):
    out[...] = out_ref[...]
    logw[...] = logw_ref[...]


def finish(out, logw):
    vmem = pl.BlockSpec(memory_space=pltpu.VMEM)
    out, logw = pl.pallas_call(
        finish_kernel,
        out_shape=(jax.ShapeDtypeStruct(out.shape, out.dtype), jax.ShapeDtypeStruct(logw.shape, logw.dtype)),
        in_specs=[vmem, vmem],
        out_specs=(vmem, vmem),
    )(out, logw)
    return (out, logw.T)


def grid_local(
    n, tokens, norm_gain, w_query, w_key, w_value, score_shift, w_conv_b, w_conv_c, w_conv_u,
    conv_kernel, w_out_att, w_out_conv,
):
    rows, d = tokens.shape
    toks = 4 * rows
    feats, att_cols = w_out_att.shape
    conv_cols = w_out_conv.shape[1]
    heads = score_shift.shape[0]
    kv_cols = w_key.shape[1]
    cells = len(CELLS)
    guests = len(CELL_BACK)
    vmem = pl.BlockSpec(memory_space=pltpu.VMEM)
    hbm = pl.BlockSpec(memory_space=pl.ANY)
    dma = pltpu.SemaphoreType.DMA
    regular = pltpu.SemaphoreType.REGULAR
    out, logw = pl.pallas_call(
        functools.partial(grid_kernel, n),
        out_shape=(
            jax.ShapeDtypeStruct((rows, n * feats), BF16),
            jax.ShapeDtypeStruct((heads, toks), F32),
        ),
        in_specs=[hbm] * 12,
        out_specs=(vmem, vmem),
        scratch_shapes=[
            pltpu.VMEM((1, d), F32),
            pltpu.VMEM((1, heads), F32),
            pltpu.VMEM(conv_kernel.shape, F32),
            pltpu.VMEM(w_query.shape, BF16),
            pltpu.VMEM((d, 2 * kv_cols), BF16),
            *[pltpu.VMEM(w.shape, BF16) for w in (w_conv_b, w_conv_c, w_conv_u)],
            pltpu.VMEM((4, rows, d), BF16),
            pltpu.VMEM((2 * rows, d), BF16),
            pltpu.VMEM((heads * toks, HEAD_DIM), BF16),
            pltpu.VMEM((n, 2, 2, 2 * rows, kv_cols), BF16),
            pltpu.VMEM((n, 2, feats, att_cols), BF16),
            pltpu.VMEM((toks, conv_cols), BF16),
            pltpu.VMEM((toks, conv_cols), BF16),
            pltpu.VMEM((HALO, conv_cols), BF16),
            pltpu.VMEM((toks + HALO, conv_cols), F32),
            pltpu.VMEM((2, 2, toks, att_cols), BF16),
            *[pltpu.VMEM((heads * toks, HEAD_DIM), F32)] * 2,
            *[pltpu.VMEM((cells, 2 * rows, feats), BF16)] * 3,
            *[pltpu.VMEM((cells, rows, feats), BF16)] * 2,
            *[pltpu.VMEM((guests, rows, feats), BF16)] * 2,
            dma((13,)), dma((5,)), dma((5,)), dma((3, n, 3)), dma((n, 3)), dma((3, n, 4)), dma((n, 4)),
            dma((2,)), dma((2, cells)), dma((2, cells)), dma((2, 2)), dma((2, guests)), regular,
        ],
        compiler_params=pltpu.CompilerParams(
            collective_id=0, has_side_effects=True, vmem_limit_bytes=60 * 1024 * 1024
        ),
    )(
        tokens, norm_gain.reshape(1, d), w_query, w_key, w_value, score_shift.reshape(1, heads),
        w_conv_b, w_conv_c, w_conv_u, conv_kernel, w_out_att, w_out_conv,
    )
    return finish(out, logw)


def solution(mesh):
    n = mesh.shape["sp"]
    body = grid_local if n == len(CELLS[0]) and mesh.shape["tp"] == 4 else local
    return jax.shard_map(
        functools.partial(body, n),
        mesh=mesh,
        in_specs=(
            P(("sp", "tp"), None), P(), P(None, "tp"), P(None, "tp"), P(None, "tp"), P("tp"),
            P(None, "tp"), P(None, "tp"), P(None, "tp"), P(None, "tp"), P("sp", "tp"), P("sp", "tp"),
        ),
        out_specs=(P(("sp", "tp"), None), P("sp", "tp")),
        check_vma=False,
    )
```
